32 devices in a mesh: sp: 8 (over z, y), tp: 4 (over x, core).
Axes of the slice: x: 2, y: 2, z: 4, core: 2. Of those that a mesh axis runs over, the one named last changes fastest.
Arguments:
- residual: bfloat16 [2048, 2048], P('sp'), may hold values from -6 to 6
- queries: bfloat16 [2048, 8, 2, 128], P('sp', 'tp'), may hold values from -100 to 100
- key_rows: bfloat16 [2048, 8, 2, 128], P('sp', 'tp'), may hold values from -6 to 6
- values: bfloat16 [2048, 8, 256], P('sp', 'tp'), may hold values from -6 to 6
- lambda_head: float32 [8], P('tp'), may hold values from 0.3 to 0.8
- sub_gain: float32 [256], replicated, may hold values from 0.1 to 1.9
- w_out: bfloat16 [2048, 2048], P('tp'), may hold values from -0.125 to 0.125
- norm_gain: float32 [2048], replicated, may hold values from 0.1 to 1.9
- w_gate: bfloat16 [2048, 5632], P('sp', 'tp'), may hold values from -0.125 to 0.125
- w_up: bfloat16 [2048, 5632], P('sp', 'tp'), may hold values from -0.125 to 0.125
- conv_gate: float32 [3, 5632], P(None, 'tp'), may hold values from -3 to 3
- conv_up: float32 [3, 5632], P(None, 'tp'), may hold values from -3 to 3
- w_down: bfloat16 [5632, 2048], P('tp'), may hold values from -0.078125 to 0.078125
Outputs:
- layer_out: bfloat16 [2048, 2048], P(('sp', 'tp'))
The draws below stay inside these ranges and needn't reach their ends.
All inputs are finite; a program needn't handle non-finite values.
Results may differ from the reference program's by a relative error of at most 0.017.
Values may be sent and summed in bfloat16 or wider, within the bound.
A program may use at most 192 MiB of HBM per device.

```python
import math
import jax
import jax.numpy as jnp
from jax import lax

D = 2048
HEADS = 8
DH = 128
DV = 256
FF = 5632
TOKENS = 2048


def query_key_pair(key):
    shape = (TOKENS, HEADS, 2, DH)
    keys_drawn = jnp.clip(1.3 * jax.random.normal(jax.random.fold_in(key, 12), shape, jnp.float32), -6.0, 6.0)
    queries_drawn = jnp.clip(1.3 * jax.random.normal(jax.random.fold_in(key, 11), shape, jnp.float32), -6.0, 6.0)
    return (queries_drawn, keys_drawn)


def draw_queries(key, part):
    return query_key_pair(key)[0].astype(jnp.bfloat16)


def draw_key_rows(key, part):
    return query_key_pair(key)[1].astype(jnp.bfloat16)


def block_scale(stream_key, extent, pieces, low, largest):
    def one(dim, shards_of):
        steps = jax.random.uniform(jax.random.fold_in(jax.random.fold_in(stream_key, 6), dim), (shards_of,), jnp.float32, low / len(pieces), largest / len(pieces))
        return jnp.repeat(jnp.exp(steps), extent[dim] // shards_of).reshape((-1,) + (1,) * (len(extent) - dim - 1))

    level = one(*pieces[0])
    for cut in pieces[1:]:
        level = level * one(*cut)
    return level


def normal_values(stream_key, dims, width, reach, split=(), held_as=jnp.bfloat16):
    result = width * jax.random.normal(stream_key, dims, jnp.float32)
    if split:
        result = result * block_scale(stream_key, dims, split, -0.22, 0.18)
    return jnp.clip(result, -reach, reach).astype(held_as)


def setup_inputs(seed: int = 0) -> dict:
    seeds = jax.random.split(jax.random.key(seed), 14)
    return {
        "residual": normal_values(seeds[0], (TOKENS, D), 1.0, 6.0, ((0, 8),)),
        "queries": draw_queries(jax.random.fold_in(seeds[13], 71), 0),
        "key_rows": draw_key_rows(jax.random.fold_in(seeds[13], 71), 0),
        "values": normal_values(seeds[3], (TOKENS, HEADS, DV), 1.0, 6.0, ((0, 8), (1, 4))),
        "lambda_head": jnp.clip(0.3 + 0.5 * jax.random.uniform(seeds[4], (HEADS,), jnp.float32) ** block_scale(seeds[4], (HEADS,), ((0, 4),), -0.2, 0.2), 0.3, 0.8),
        "sub_gain": jnp.clip(1.0 + 0.18 * jax.random.normal(seeds[5], (DV,), jnp.float32), 0.1, 1.9),
        "w_out": normal_values(seeds[6], (HEADS * DV, D), (HEADS * DV) ** -0.5, 0.125, ((0, 4),)),
        "norm_gain": jnp.clip(1.0 + 0.18 * jax.random.normal(seeds[7], (D,), jnp.float32), 0.1, 1.9),
        "w_gate": normal_values(seeds[8], (D, FF), D ** -0.5, 0.125, ((0, 8), (1, 4))),
        "w_up": normal_values(seeds[9], (D, FF), D ** -0.5, 0.125, ((0, 8), (1, 4))),
        "conv_gate": normal_values(seeds[10], (3, FF), 0.577, 3.0, ((1, 4),), jnp.float32),
        "conv_up": normal_values(seeds[11], (3, FF), 0.577, 3.0, ((1, 4),), jnp.float32),
        "w_down": normal_values(seeds[12], (FF, D), FF ** -0.5, 0.078125, ((0, 4),)),
    }


epsilon = 1e-06
lambda_init = 0.8 - 0.6 * math.exp(-0.3)

def causal_mix(rows_in, taps):
    padded_rows = jnp.concatenate([jnp.zeros((2, rows_in.shape[1]), jnp.float32), rows_in.astype(jnp.float32)], 0)
    return taps[0] * padded_rows[:-2] + taps[1] * padded_rows[1:-1] + taps[2] * padded_rows[2:]

def reference(residual, queries, key_rows, values, lambda_head, sub_gain, w_out, norm_gain, w_gate, w_up, conv_gate, conv_up, w_down):
    query_block = math.gcd(TOKENS, 256)
    score_scale = 1.0 / math.sqrt(DH)
    key_pos = jnp.arange(TOKENS, dtype=jnp.int32)
    keys_wide = key_rows.astype(jnp.float32)
    values_wide = values.astype(jnp.float32)

    def attend(block_start):
        query_part = lax.dynamic_slice_in_dim(queries, block_start, query_block, 0).astype(jnp.float32)
        scores = jnp.einsum('qhcd,khcd->hcqk', query_part, keys_wide) * score_scale
        query_pos = block_start + jnp.arange(query_block, dtype=jnp.int32)
        causal_mask = key_pos[None, :] <= query_pos[:, None]
        scores = jnp.where(causal_mask, scores, -1e+30)
        run_max = lax.optimization_barrier(jnp.max(scores, axis=-1, keepdims=True))
        weights = jnp.where(causal_mask, jnp.exp(scores - run_max), 0.0)
        run_sum = lax.optimization_barrier(jnp.sum(weights, axis=-1))
        rounded = lax.optimization_barrier(weights.astype(jnp.bfloat16)).astype(jnp.float32)
        summed = jnp.einsum('hcqk,khe->hcqe', rounded, values_wide)
        blended = summed / run_sum[..., None]
        return blended[:, 0] - lambda_head[:, None, None] * blended[:, 1]
    starts = (jnp.arange(TOKENS // query_block, dtype=jnp.int32) * query_block).astype(jnp.int32)
    attended = lax.map(attend, starts)
    attended = jnp.transpose(attended, (0, 2, 1, 3)).reshape(TOKENS, HEADS, DV)
    mean_square = lax.optimization_barrier(jnp.mean(attended * attended, axis=-1, keepdims=True))
    normed = attended * lax.rsqrt(mean_square + epsilon) * sub_gain * (1.0 - lambda_init)
    normed = normed.astype(jnp.bfloat16).reshape(TOKENS, HEADS * DV)
    middle = residual.astype(jnp.float32) + jnp.dot(normed, w_out, preferred_element_type=jnp.float32)
    row_square = lax.optimization_barrier(jnp.mean(middle * middle, axis=-1, keepdims=True))
    normed_rows = (middle * lax.rsqrt(row_square + epsilon) * norm_gain).astype(jnp.bfloat16)
    gate_pre = jnp.dot(normed_rows, w_gate, preferred_element_type=jnp.float32).astype(jnp.bfloat16)
    up_pre = jnp.dot(normed_rows, w_up, preferred_element_type=jnp.float32).astype(jnp.bfloat16)
    gate_mixed = causal_mix(gate_pre, conv_gate)
    up_mixed = causal_mix(up_pre, conv_up)
    hidden = (jax.nn.silu(gate_mixed) * up_mixed).astype(jnp.bfloat16)
    lowered = jnp.dot(hidden, w_down, preferred_element_type=jnp.float32)
    return (middle + lowered).astype(jnp.bfloat16)
```

```python
import contextlib
import functools
import math

import jax
import jax.numpy as jnp
from jax import lax
from jax.experimental import pallas as pl
from jax.experimental.pallas import tpu as pltpu
from jax.sharding import PartitionSpec as P

MESH = pl.DeviceIdType.MESH
epsilon = 1e-06
lambda_init = 0.8 - 0.6 * math.exp(-0.3)
bf16 = jnp.bfloat16
f32 = jnp.float32
HALO = 16
GROUP = 4
HUBS = (1, 2)
LANES = 128


def scope(name):
    return contextlib.nullcontext()


def parts_of(units):
    chunks = units // LANES
    first = (chunks + 1) // 2
    return ((0, first * LANES), (first * LANES, (chunks - first) * LANES))


def kernel(
    S, T, heads, dh, dv,
    q_hbm, kv_hbm, res_hbm, wout_hbm, wg_hbm, wu_hbm, wd_hbm,
    lam_ref, sub_ref, norm_ref, cg_ref, cu_ref,
    out_ref,
    q, kv, res, wout, wg, wu, wd, stage,
    m_s, l_s, acc_s, n_own, n_in, part, part_in, mid, hn,
    g_s, u_s, halo_out, halo_in, hid, low, low_in, half, half_in, done, ret,
    local_sem, own_sem, pair_sem, kv_send, kv_recv,
    w_send, w_recv, cross_send, stage_recv, stage_send, relay_send,
    tp_send, tp_recv, hn_send, hn_recv, ag_send, ag_recv,
    halo_send, halo_recv, core_send, core_recv, far_send, far_recv, ret_send, ret_recv,
):
    Z = S // 2
    sp = lax.axis_index("sp")
    tp = lax.axis_index("tp")
    z = lax.div(sp, 2)
    y = lax.rem(sp, 2)
    zi = lax.rem(z, GROUP)
    base = z - zi
    rows = q.shape[1]
    feat, units = wg_hbm.shape
    hh = heads // 2
    kw = 2 * hh * dh
    D = wout.shape[1]
    own = rows // T
    cap = wg.shape[1]
    pieces = parts_of(units)
    other = 1 - y
    mate = z * 2 + other
    has_up = z < Z - 1
    hub = (zi == HUBS[0]) | (zi == HUBS[1])
    near = jnp.where(zi == HUBS[0], z - 1, z + 1)
    core_mate = tp + 1 - 2 * lax.rem(tp, 2)
    far_mate = lax.rem(tp + 2, T)
    diagonal = T - 1 - tp

    def one(flag):
        return flag.astype(jnp.int32)

    def peer(d):
        return lax.rem(tp + d, T)

    def remote(src, dst, send, recv, device):
        return pltpu.make_async_remote_copy(
            src_ref=src, dst_ref=dst, send_sem=send, recv_sem=recv, device_id=device, device_id_type=MESH
        )

    def cols(k):
        return pl.ds(pieces[k][0], pieces[k][1])

    def block(b, k):
        return (pl.ds(pl.multiple_of(b * feat, feat), feat), pl.ds(0, pieces[k][1]))

    sources, stores = (wg_hbm, wu_hbm), (wg, wu)
    targets = [(g * GROUP + HUBS[k], k) for g in range(Z // GROUP) for k in range(2)]

    def direct(i, w):
        h, k = targets[i]
        return remote(
            sources[w].at[:, cols(k)], stores[w].at[block(sp, k)],
            w_send.at[w, i], w_recv.at[w, sp], (h * 2 + y, tp),
        )

    def cross(k, w):
        return remote(
            sources[w].at[:, cols(k)], stores[w].at[block(sp, k)],
            cross_send.at[w], w_recv.at[w, sp], (mate, tp),
        )

    def lend(k, w):
        return remote(
            sources[w].at[:, cols(k)], stage.at[w, :, pl.ds(0, pieces[k][1])],
            cross_send.at[w], stage_recv.at[w], (mate, tp),
        )

    def pass_on(k, w):
        h = base + HUBS[k]
        return remote(
            stage.at[w, :, pl.ds(0, pieces[k][1])], stores[w].at[block(mate, k)],
            stage_send.at[w], w_recv.at[w, mate], (h * 2 + y, tp),
        )

    def relay(zz, k, w):
        b = zz * 2 + y
        return remote(
            stores[w].at[block(b, k)], stores[w].at[block(b, k)],
            relay_send.at[w, zz], w_recv.at[w, b], (mate, tp),
        )

    def own_piece(k, w):
        return pltpu.make_async_copy(sources[w].at[:, cols(k)], stores[w].at[block(sp, k)], own_sem.at[w])

    def down_piece(k):
        return pltpu.make_async_copy(
            wd_hbm.at[cols(k), :], wd.at[pl.ds(0, pieces[k][1]), :], own_sem.at[2]
        )

    def as_hub(fn):
        for k in range(2):
            pl.when(zi == HUBS[k])(functools.partial(fn, k))

    def as_outer(fn):
        for k, zo in ((0, 0), (1, 3)):
            pl.when(zi == zo)(functools.partial(fn, k))

    loads = [
        pltpu.make_async_copy(kv_hbm.at[y], kv.at[sp], local_sem.at[0]),
        pltpu.make_async_copy(q_hbm.at[y], q.at[y], local_sem.at[1]),
        pltpu.make_async_copy(wout_hbm, wout, local_sem.at[2]),
        pltpu.make_async_copy(res_hbm.at[pl.ds(pl.multiple_of(tp * own, own), own), :], res, local_sem.at[3]),
    ]
    for c in loads:
        c.start()

    def load_pieces(k):
        own_piece(k, 0).start()
        own_piece(k, 1).start()
        down_piece(k).start()

    as_hub(load_pieces)

    barrier = pltpu.get_barrier_semaphore()
    next_group, prev_group = (y == 1) & (z + GROUP < Z), (y == 0) & (z >= GROUP)

    def greet(device):
        pl.semaphore_signal(barrier, inc=1, device_id=device, device_id_type=MESH)

    with scope("barrier"):
        for zz in range(Z):
            pl.when(z != zz)(functools.partial(greet, (zz * 2 + y, tp)))
        greet((mate, tp))
        for d in range(1, T):
            greet((sp, peer(d)))
        pl.when(next_group)(lambda: greet((sp + 2 * GROUP - 1, tp)))
        pl.when(prev_group)(lambda: greet((sp - 2 * GROUP + 1, tp)))
        pl.semaphore_wait(barrier, Z + T - 1 + one(next_group) + one(prev_group))

    def climb(blk):
        return remote(kv.at[blk], kv.at[blk], kv_send.at[blk], kv_recv.at[blk], (sp + 2, tp))

    def send_up(blk):
        pl.when(has_up)(lambda: climb(blk).start())

    def pair(src, dst, k):
        return remote(src, dst, pair_sem.at[0, k], pair_sem.at[1, k], (mate, tp))

    kv_swap = pair(kv_hbm.at[other], kv.at[sp], 0)
    q_swap = pair(q_hbm.at[other], q.at[y], 1)
    kv_got = pair(kv_hbm.at[other], kv.at[mate], 0)
    q_got = pair(q_hbm.at[other], q.at[other], 1)
    kv_swap.start()
    q_swap.start()
    loads[0].wait()
    send_up(sp)

    def direct_send(i):
        direct(i, 0).start()
        direct(i, 1).start()

    for i in reversed(range(len(targets))):
        pl.when(z > targets[i][0])(functools.partial(direct_send, i))

    def early(h):
        return (zi == 0) & (h == z + 1)

    for i in range(len(targets)):
        pl.when(early(targets[i][0]))(lambda: direct(i, 0).start())

    def cross_start(k):
        cross(k, 0).start()
        cross(k, 1).start()

    def lend_start(k):
        lend(k, 0).start()
        lend(k, 1).start()

    as_hub(cross_start)
    as_outer(lend_start)

    def forward_staged(k):
        for w in range(2):
            lend(k, w).wait_recv()
            pass_on(k, w).start()

    loads[1].wait()

    m_s[...] = jnp.full(m_s.shape, -1e30, f32)
    l_s[...] = jnp.zeros(l_s.shape, f32)
    acc_s[...] = jnp.zeros(acc_s.shape, f32)
    scale = 1.0 / math.sqrt(dh)

    def clear_tail(k):
        lo, wide = pieces[k][1], cap - pieces[k][1]
        if wide:
            wg[:, lo:] = jnp.zeros((D, wide), bf16)
            wu[:, lo:] = jnp.zeros((D, wide), bf16)
            wd[lo:, :] = jnp.zeros((wide, D), bf16)

    as_hub(clear_tail)

    def attend(yy, blk):
        row_at = (z * 2 + yy) * rows + lax.broadcasted_iota(jnp.int32, (rows, rows), 0)
        col_at = blk * rows + lax.broadcasted_iota(jnp.int32, (rows, rows), 1)
        keep = col_at <= row_at
        for h in range(hh):
            v = kv[blk, :, kw + h * dv : kw + (h + 1) * dv]
            for c in range(2):
                i = 2 * h + c
                k = kv[blk, :, i * dh : (i + 1) * dh]
                s = lax.dot_general(
                    q[yy, :, i * dh : (i + 1) * dh], k, (((1,), (1,)), ((), ())),
                    preferred_element_type=f32,
                ) * scale
                s = jnp.where(keep, s, -1e30)
                old = m_s[yy, i]
                new = jnp.maximum(old, jnp.max(s, axis=1, keepdims=True))
                e = jnp.where(keep, jnp.exp(s - new), 0.0)
                fade = jnp.exp(old - new)
                m_s[yy, i] = new
                l_s[yy, i] = l_s[yy, i] * fade + jnp.sum(e, axis=1, keepdims=True)
                acc_s[yy, i] = acc_s[yy, i] * fade + jnp.dot(
                    e.astype(bf16), v, preferred_element_type=f32
                )

    with scope("kvgot"):
        kv_got.wait_recv()
        send_up(mate)
        q_got.wait_recv()

    @pl.loop(0, Z)
    def _(r):
        @pl.when(z >= r)
        def _():
            @pl.when(r > 0)
            def _():
                for blk in (sp - 2 * r, mate - 2 * r):
                    with scope("arrkv"):
                        climb(blk).wait_recv()
                    send_up(blk)

            @pl.loop(0, 4)
            def _(i):
                yy, c = lax.div(i, 2), lax.rem(i, 2)
                with scope("attend"):
                    pl.when((r > 0) | (yy >= c))(lambda: attend(yy, (z - r) * 2 + c))

            pl.when((r == 2) & (zi == 3))(lambda: forward_staged(1))

    for i in range(len(targets)):
        h = targets[i][0]
        pl.when((z < h) & jnp.logical_not(early(h)))(lambda: direct(i, 0).start())
        pl.when(z < h)(lambda: direct(i, 1).start())

    def relayed(zz):
        return (zz != z) & (zz != near)

    def relay_from(zz):
        @pl.when(relayed(zz))
        def _():
            def go(k):
                for w in range(2):
                    relay(zz, k, w).wait_recv()
                    relay(zz, k, w).start()

            as_hub(go)

    with scope("nnorm"):
        for yy in range(2):
            for h in range(hh):
                a0 = acc_s[yy, 2 * h] / l_s[yy, 2 * h]
                a1 = acc_s[yy, 2 * h + 1] / l_s[yy, 2 * h + 1]
                a = a0 - lam_ref[y * hh + h] * a1
                ms = jnp.mean(a * a, axis=1, keepdims=True)
                n = a * lax.rsqrt(ms + epsilon) * sub_ref[...] * (1.0 - lambda_init)
                n_own[yy, :, h * dv : (h + 1) * dv] = n.astype(bf16)
    n_swap = pair(n_own.at[other], n_in, 2)
    n_swap.start()
    with scope("relay1"):
        pl.when(zi == HUBS[0])(lambda: relay_from(z + 1))
    with scope("nswapw"):
        loads[2].wait()
        n_swap.wait_recv()
    width = min(512, D)
    hw = hh * dv
    with scope("outproj"):
        for c in range(0, D, width):
            at = slice(c, c + width)
            part[:, :, at] = (
                (
                    jnp.dot(n_own[y], wout[pl.ds(y * hw, hw), at], preferred_element_type=f32)
                    + jnp.dot(n_in[...], wout[pl.ds(other * hw, hw), at], preferred_element_type=f32)
                )
                .astype(bf16)
                .reshape(T, own, width)
            )

    def swap(d):
        return remote(part.at[peer(d)], part_in.at[d], tp_send.at[d], tp_recv.at[d], (sp, peer(d)))

    firsts = [swap(d) for d in range(1, T)]
    for c in firsts:
        c.start()
    with scope("rs1"):
        loads[3].wait()
        total = res[...].astype(f32) + part[tp].astype(f32)
        for d in range(1, T):
            firsts[d - 1].wait_recv()
            total = total + part_in[d].astype(f32)
        mid[...] = total
        ms = jnp.mean(total * total, axis=1, keepdims=True)

    def slot(p, t):
        return hn.at[p, pl.ds(pl.multiple_of(t * own, own), own)]

    hn[zi, pl.ds(pl.multiple_of(tp * own, own), own), :] = (
        total * lax.rsqrt(ms + epsilon) * norm_ref[...]
    ).astype(bf16)

    def deliver(k):
        return remote(
            slot(zi, tp), slot(zi, tp), hn_send.at[k], hn_recv.at[zi], ((base + HUBS[k]) * 2 + y, tp)
        )

    pl.when(zi < 2)(lambda: deliver(1).start())
    pl.when(zi != HUBS[0])(lambda: deliver(0).start())
    pl.when(zi == 3)(lambda: deliver(1).start())
    pl.when(zi == 0)(lambda: forward_staged(0))

    with scope("relay2"):
        pl.when(zi == HUBS[0])(lambda: pl.loop(z + 2, Z)(relay_from))
        pl.when(zi == HUBS[1])(lambda: pl.loop(z + 2, Z)(relay_from))

        @pl.when(hub)
        def _():
            @pl.loop(0, z)
            def _(i):
                relay_from(z - 1 - i)

    def spread(p, hop):
        src = (tp, tp, far_mate)[hop]
        to = (far_mate, core_mate, core_mate)[hop]
        return remote(slot(p, src), slot(p, src), ag_send.at[p, hop], ag_recv.at[p, hop], (sp, to))

    def gather1(p):
        @pl.when(p != zi)
        def _():
            remote(slot(p, tp), slot(p, tp), hn_send.at[0], hn_recv.at[p], (sp, tp)).wait_recv()

        spread(p, 0).start()
        spread(p, 1).start()

    def gather2(p):
        spread(p, 0).wait_recv()
        spread(p, 2).start()

    def halo_copy(p):
        last = (y == 1) & (p == GROUP - 1)
        to = jnp.where(last, sp + 2 * GROUP - 1, mate)
        nxt = jnp.where(last, 0, p + y)
        return remote(
            halo_out.at[p], halo_in.at[nxt], halo_send.at[p], halo_recv.at[nxt], (to, tp)
        )

    def halo_sends(p):
        return (y == 0) | (p < GROUP - 1) | (z + GROUP < Z)

    def core_copy(p, i):
        return remote(
            low.at[p, (core_mate, diagonal)[i]], low_in.at[p, i], core_send.at[p, i], core_recv.at[p, i],
            (sp, core_mate),
        )

    def far_copy(p):
        return remote(half.at[p], half_in.at[p], far_send.at[p], far_recv.at[p], (sp, far_mate))

    def give_back(p, k):
        return remote(done.at[p], ret.at[k], ret_send.at[p], ret_recv.at[k], ((base + p) * 2 + y, tp))

    def feed(p):
        wide = 256
        for c in range(0, cap, wide):
            at = slice(c, c + wide)
            g_s[HALO:, at] = jnp.dot(hn[p], wg[:, at], preferred_element_type=f32).astype(bf16).astype(f32)
            u_s[HALO:, at] = jnp.dot(hn[p], wu[:, at], preferred_element_type=f32).astype(bf16).astype(f32)
        halo_out[p, 0] = g_s[rows:, :].astype(bf16)
        halo_out[p, 1] = u_s[rows:, :].astype(bf16)
        pl.when(halo_sends(p))(lambda: halo_copy(p).start())
        first = (y == 0) & (p == 0) & (base == 0)

        @pl.when(first)
        def _():
            g_s[:HALO, :] = jnp.zeros((HALO, cap), f32)
            u_s[:HALO, :] = jnp.zeros((HALO, cap), f32)

        @pl.when(jnp.logical_not(first))
        def _():
            remote(halo_out.at[p], halo_in.at[p], halo_send.at[p], halo_recv.at[p], (mate, tp)).wait_recv()
            g_s[:HALO, :] = halo_in[p, 0].astype(f32)
            u_s[:HALO, :] = halo_in[p, 1].astype(f32)

        lo = jnp.where(zi == HUBS[0], pieces[0][0], pieces[1][0])
        for c in range(0, cap, LANES):
            at = slice(c, c + LANES)
            tap = pl.ds(pl.multiple_of(jnp.minimum(lo + c, units - LANES), LANES), LANES)

            def mix(x, taps):
                out = taps[0:1, tap] * x[HALO - 2 : HALO - 2 + rows, at]
                out = out + taps[1:2, tap] * x[HALO - 1 : HALO - 1 + rows, at]
                return out + taps[2:3, tap] * x[HALO:, at]

            gm, um = mix(g_s, cg_ref), mix(u_s, cu_ref)
            hid[:, at] = (gm / (1.0 + jnp.exp(-gm)) * um).astype(bf16)
        for c in range(0, D, width):
            at = slice(c, c + width)
            low[p, :, :, at] = (
                jnp.dot(hid[...], wd[:, at], preferred_element_type=f32).astype(bf16).reshape(T, own, width)
            )
        core_copy(p, 1).start()
        core_copy(p, 0).start()

    def reduce1(p):
        core_copy(p, 1).wait_recv()
        half[p] = (low[p, far_mate].astype(f32) + low_in[p, 1].astype(f32)).astype(bf16)
        far_copy(p).start()

    def reduce2(p):
        core_copy(p, 0).wait_recv()
        far_copy(p).wait_recv()
        t = low[p, tp].astype(f32) + low_in[p, 0].astype(f32) + half_in[p].astype(f32)

        def hand(k):
            @pl.when(p == zi)
            def _():
                ret[k] = t.astype(bf16)

            @pl.when(p != zi)
            def _():
                done[p] = t.astype(bf16)
                give_back(p, k).start()

        as_hub(hand)

    def wait_pieces(k):
        for w in range(2):
            own_piece(k, w).wait()

            def arrived(b):
                remote(
                    stores[w].at[block(b, k)], stores[w].at[block(b, k)],
                    cross_send.at[w], w_recv.at[w, b], (mate, tp),
                ).wait_recv()

            arrived(near * 2 + y)

            @pl.loop(0, Z)
            def _(zz):
                arrived(zz * 2 + other)

        down_piece(k).wait()

    @pl.when(hub)
    def _():
        with scope("gather"):
            for p in range(3):
                gather1(p)
                gather2(p)

        with scope("wwait"):
            as_hub(wait_pieces)

        @pl.loop(0, GROUP)
        def _(p):
            @pl.when(p == GROUP - 2)
            def _():
                with scope("gather3"):
                    gather1(GROUP - 1)

            @pl.when(p == GROUP - 1)
            def _():
                with scope("gather4"):
                    gather2(GROUP - 1)

            with scope("agw"):
                spread(p, 1).wait_recv()
                spread(p, 2).wait_recv()
            with scope("feed"):
                feed(p)

            @pl.when((p > 0) & (p < GROUP - 1))
            def _():
                with scope("red"):
                    reduce1(p - 1)

        with scope("redlast"):
            reduce1(GROUP - 2)
            reduce2(0)
            reduce1(GROUP - 1)
            for p in range(1, GROUP):
                reduce2(p)

    with scope("final"):
        total = mid[...]
        for k in range(2):
            pl.when(zi != HUBS[k])(
                lambda: remote(done.at[0], ret.at[k], ret_send.at[0], ret_recv.at[k], (sp, tp)).wait_recv()
            )
            total = total + ret[k].astype(f32)
        out_ref[...] = total.astype(bf16)

    with scope("drain"):
        @pl.loop(0, Z)
        def _(zz):
            @pl.when(has_up & (zz <= z))
            def _():
                climb(2 * zz).wait_send()
                climb(2 * zz + 1).wait_send()

            @pl.when(hub & relayed(zz))
            def _():
                def go(k):
                    relay(zz, k, 0).wait_send()
                    relay(zz, k, 1).wait_send()

                as_hub(go)

        for i in range(len(targets)):
            @pl.when(z != targets[i][0])
            def _():
                direct(i, 0).wait_send()
                direct(i, 1).wait_send()

        def cross_end(k):
            cross(k, 0).wait_send()
            cross(k, 1).wait_send()

        def lend_end(k):
            for w in range(2):
                lend(k, w).wait_send()
                pass_on(k, w).wait_send()

        as_hub(cross_end)
        as_outer(lend_end)
        for c in firsts + [kv_swap, q_swap, n_swap]:
            c.wait_send()
        for k in range(2):
            pl.when(zi != HUBS[k])(lambda: deliver(k).wait_send())

        @pl.when(hub)
        def _():
            @pl.loop(0, GROUP)
            def _(p):
                for hop in range(3):
                    spread(p, hop).wait_send()
                pl.when(halo_sends(p))(lambda: halo_copy(p).wait_send())
                core_copy(p, 0).wait_send()
                core_copy(p, 1).wait_send()
                far_copy(p).wait_send()
                pl.when(p != zi)(lambda: give_back(p, 0).wait_send())


def local(
    S, T,
    residual, queries, key_rows, values, lambda_head, sub_gain, w_out, norm_gain,
    w_gate, w_up, conv_gate, conv_up, w_down,
):
    rows, heads, maps, dh = queries.shape
    dv = values.shape[2]
    feat, units = w_gate.shape
    D = w_out.shape[1]
    own = rows // T
    cap = max(p[1] for p in parts_of(units))
    hh = heads // 2
    q = queries.reshape(rows, 2, hh * maps * dh).swapaxes(0, 1)
    kv = jnp.concatenate(
        [key_rows.reshape(rows, 2, hh * maps * dh), values.reshape(rows, 2, hh * dv)], axis=2
    ).swapaxes(0, 1)
    kvw = kv.shape[2]
    Z = S // 2
    hbm = pl.BlockSpec(memory_space=pl.ANY)
    vmem = pl.BlockSpec(memory_space=pltpu.VMEM)
    smem = pl.BlockSpec(memory_space=pltpu.SMEM)
    V = pltpu.VMEM
    dma = pltpu.SemaphoreType.DMA
    return pl.pallas_call(
        functools.partial(kernel, S, T, heads, dh, dv),
        out_shape=jax.ShapeDtypeStruct((own, D), bf16),
        in_specs=[hbm] * 7 + [smem] + [vmem] * 4,
        out_specs=vmem,
        scratch_shapes=[
            V(q.shape, bf16),
            V((S, rows, kvw), bf16),
            V((own, D), bf16),
            V(w_out.shape, bf16),
            V((D, cap), bf16),
            V((D, cap), bf16),
            V((cap, D), bf16),
            V((2, feat, cap), bf16),
            V((2, 2 * hh, rows, 1), f32),
            V((2, 2 * hh, rows, 1), f32),
            V((2, 2 * hh, rows, dv), f32),
            V((2, rows, hh * dv), bf16),
            V((rows, hh * dv), bf16),
            V((T, own, D), bf16),
            V((T, own, D), bf16),
            V((own, D), f32),
            V((GROUP, rows, D), bf16),
            V((rows + HALO, cap), f32),
            V((rows + HALO, cap), f32),
            V((GROUP, 2, HALO, cap), bf16),
            V((GROUP, 2, HALO, cap), bf16),
            V((rows, cap), bf16),
            V((GROUP, T, own, D), bf16),
            V((GROUP, 2, own, D), bf16),
            V((GROUP, own, D), bf16),
            V((GROUP, own, D), bf16),
            V((GROUP, own, D), bf16),
            V((2, own, D), bf16),
            dma((4,)),
            dma((3,)),
            dma((2, 3)),
            dma((S,)),
            dma((S,)),
            dma((2, Z // 2)),
            dma((2, S)),
            dma((2,)),
            dma((2,)),
            dma((2,)),
            dma((2, Z)),
            dma((T,)),
            dma((T,)),
            dma((2,)),
            dma((GROUP,)),
            dma((GROUP, 3)),
            dma((GROUP, 3)),
            dma((GROUP,)),
            dma((GROUP,)),
            dma((GROUP, 2)),
            dma((GROUP, 2)),
            dma((GROUP,)),
            dma((GROUP,)),
            dma((GROUP,)),
            dma((2,)),
        ],
        compiler_params=pltpu.CompilerParams(
            collective_id=0, has_side_effects=True, vmem_limit_bytes=64000000
        ),
    )(
        q, kv, residual, w_out, w_gate, w_up, w_down, lambda_head,
        sub_gain.reshape(1, -1), norm_gain.reshape(1, -1), conv_gate, conv_up,
    )


def solution(mesh):
    placed = (
        P("sp", None),
        P("sp", "tp", None, None),
        P("sp", "tp", None, None),
        P("sp", "tp", None),
        P("tp"),
        P(),
        P("tp", None),
        P(),
        P("sp", "tp"),
        P("sp", "tp"),
        P(None, "tp"),
        P(None, "tp"),
        P("tp", None),
    )
    return jax.shard_map(
        functools.partial(local, mesh.shape["sp"], mesh.shape["tp"]),
        mesh=mesh, in_specs=placed, out_specs=P(("sp", "tp"), None), check_vma=False,
    )
```

```python
import contextlib
import functools
import math

import jax
import jax.numpy as jnp
from jax import lax
from jax.experimental import pallas as pl
from jax.experimental.pallas import tpu as pltpu
from jax.sharding import PartitionSpec as P

MESH = pl.DeviceIdType.MESH
epsilon = 1e-06
lambda_init = 0.8 - 0.6 * math.exp(-0.3)
bf16 = jnp.bfloat16
f32 = jnp.float32
HALO = 16
GROUP = 4
HUBS = (1, 2)
LANES = 128
SPLIT = 2
STAGED = {3: ((1, 0), (0, 0), (0, 1))}


def scope(name):
    return contextlib.nullcontext()


def parts_of(units):
    chunks = units // LANES
    first = (chunks + 1) // 2
    return ((0, first * LANES), (first * LANES, (chunks - first) * LANES))


def kernel(
    S, T, heads, dh, dv,
    q_hbm, k_hbm, v_hbm, res_hbm, wout_hbm, wg_hbm, wu_hbm, wd_hbm,
    lam_ref, sub_ref, norm_ref, cg_ref, cu_ref,
    out_ref,
    q_raw, k_raw, v_raw, q_out, kv_out, q, kv, res, wout, wg, wu, wd, stage,
    m_s, l_s, acc_s, n_own, n_in, part, part_in, mid, hn,
    g_s, u_s, halo_out, halo_in, hid, low, low_in, half, half_in, done, ret,
    local_sem, own_sem, pair_sem, kv_send, kv_recv,
    w_send, w_recv, cross_send, lend_send, stage_recv, stage_send, relay_send,
    tp_send, tp_recv, hn_send, hn_recv, ag_send, ag_recv,
    halo_send, halo_recv, core_send, core_recv, far_send, far_recv, ret_send, ret_recv,
):
    Z = S // 2
    sp = lax.axis_index("sp")
    tp = lax.axis_index("tp")
    z = lax.div(sp, 2)
    y = lax.rem(sp, 2)
    zi = lax.rem(z, GROUP)
    base = z - zi
    rows = q.shape[1]
    feat, units = wg_hbm.shape
    hh = heads // 2
    kw = 2 * hh * dh
    D = wout.shape[1]
    own = rows // T
    cap = wg.shape[1]
    pieces = parts_of(units)
    other = 1 - y
    mate = z * 2 + other
    has_up = z < Z - 1
    hub = (zi == HUBS[0]) | (zi == HUBS[1])
    core_mate = tp + 1 - 2 * lax.rem(tp, 2)
    far_mate = lax.rem(tp + 2, T)
    diagonal = T - 1 - tp

    def one(flag):
        return flag.astype(jnp.int32)

    def peer(d):
        return lax.rem(tp + d, T)

    def remote(src, dst, send, recv, device):
        return pltpu.make_async_remote_copy(
            src_ref=src, dst_ref=dst, send_sem=send, recv_sem=recv, device_id=device, device_id_type=MESH
        )

    def cols(k):
        return pl.ds(pieces[k][0], pieces[k][1])

    def block(b, k):
        return (pl.ds(pl.multiple_of(b * feat, feat), feat), pl.ds(0, pieces[k][1]))

    sources, stores = (wg_hbm, wu_hbm), (wg, wu)
    targets = [(g * GROUP + HUBS[k], k) for g in range(Z // GROUP) for k in range(2)]

    def direct(i, w):
        h, k = targets[i]
        return remote(
            sources[w].at[:, cols(k)], stores[w].at[block(sp, k)],
            w_send.at[w, i], w_recv.at[w, sp], (h * 2 + y, tp),
        )

    def cross(k, w):
        return remote(
            sources[w].at[:, cols(k)], stores[w].at[block(sp, k)],
            cross_send.at[w], w_recv.at[w, sp], (mate, tp),
        )

    def lend(k, w):
        return remote(
            sources[w].at[:, cols(k)], stage.at[k, w, :, pl.ds(0, pieces[k][1])],
            lend_send.at[k, w], stage_recv.at[k, w], (mate, tp),
        )

    def pass_on(k, w):
        h = base + HUBS[k]
        return remote(
            stage.at[k, w, :, pl.ds(0, pieces[k][1])], stores[w].at[block(mate, k)],
            stage_send.at[k, w], w_recv.at[w, mate], (h * 2 + y, tp),
        )

    def staged(zz, k, w):
        hit = zz < 0
        for zo, which in STAGED.items():
            if (k, w) in which:
                hit = hit | (zz == base + zo)
        return hit

    def each_staged(fn):
        for zo, which in STAGED.items():
            for k, w in which:
                pl.when(zi == zo)(functools.partial(fn, k, w))

    def relay(zz, k, w):
        b = zz * 2 + y
        return remote(
            stores[w].at[block(b, k)], stores[w].at[block(b, k)],
            relay_send.at[w, zz], w_recv.at[w, b], (mate, tp),
        )

    def own_piece(k, w):
        return pltpu.make_async_copy(sources[w].at[:, cols(k)], stores[w].at[block(sp, k)], own_sem.at[w])

    def down_piece(k):
        return pltpu.make_async_copy(
            wd_hbm.at[cols(k), :], wd.at[pl.ds(0, pieces[k][1]), :], own_sem.at[2]
        )

    def as_hub(fn):
        for k in range(2):
            pl.when(zi == HUBS[k])(functools.partial(fn, k))

    loads = [
        pltpu.make_async_copy(k_hbm, k_raw, local_sem.at[0]),
        pltpu.make_async_copy(v_hbm, v_raw, local_sem.at[4]),
        pltpu.make_async_copy(q_hbm, q_raw, local_sem.at[1]),
        pltpu.make_async_copy(wout_hbm, wout, local_sem.at[2]),
        pltpu.make_async_copy(res_hbm.at[pl.ds(pl.multiple_of(tp * own, own), own), :], res, local_sem.at[3]),
    ]
    for c in loads:
        c.start()

    def load_pieces(k):
        own_piece(k, 0).start()
        own_piece(k, 1).start()
        down_piece(k).start()

    as_hub(load_pieces)

    barrier = pltpu.get_barrier_semaphore()
    next_group, prev_group = (y == 1) & (z + GROUP < Z), (y == 0) & (z >= GROUP)

    def greet(device):
        pl.semaphore_signal(barrier, inc=1, device_id=device, device_id_type=MESH)

    with scope("barrier"):
        for zz in range(Z):
            pl.when(z != zz)(functools.partial(greet, (zz * 2 + y, tp)))
        greet((mate, tp))
        for d in range(1, T):
            greet((sp, peer(d)))
        pl.when(next_group)(lambda: greet((sp + 2 * GROUP - 1, tp)))
        pl.when(prev_group)(lambda: greet((sp - 2 * GROUP + 1, tp)))
        with scope("relayout"):
            for c in loads[:3]:
                c.wait()
            for yy in range(2):
                @pl.when(y == yy)
                def _():
                    for mine, q_to, kv_to in ((True, q.at[y], kv.at[sp]), (False, q_out, kv_out)):
                        for h in range(hh):
                            head = (yy if mine else 1 - yy) * hh + h
                            for c in range(2):
                                i = 2 * h + c
                                q_to[:, i * dh : (i + 1) * dh] = q_raw[:, head, c, :]
                                kv_to[:, i * dh : (i + 1) * dh] = k_raw[:, head, c, :]
                            kv_to[:, kw + h * dv : kw + (h + 1) * dv] = v_raw[:, head, :]
        pl.semaphore_wait(barrier, Z + T - 1 + one(next_group) + one(prev_group))

    def climb(blk):
        return remote(kv.at[blk], kv.at[blk], kv_send.at[blk], kv_recv.at[blk], (sp + 2, tp))

    def send_up(blk):
        pl.when(has_up)(lambda: climb(blk).start())

    def pair(src, dst, k):
        return remote(src, dst, pair_sem.at[0, k], pair_sem.at[1, k], (mate, tp))

    kv_swap = pair(kv_out, kv.at[sp], 0)
    q_swap = pair(q_out, q.at[y], 1)
    kv_got = pair(kv_out, kv.at[mate], 0)
    q_got = pair(q_out, q.at[other], 1)
    kv_swap.start()
    q_swap.start()
    send_up(sp)

    def direct_send(i):
        direct(i, 0).start()
        direct(i, 1).start()

    for i in reversed(range(len(targets))):
        pl.when(z > targets[i][0])(functools.partial(direct_send, i))

    def early(h):
        return (zi == 1) & (h == z + 1)

    for i in range(len(targets)):
        pl.when(early(targets[i][0]))(lambda: direct(i, 0).start())

    def cross_start(k):
        cross(k, 0).start()
        cross(k, 1).start()

    as_hub(cross_start)
    each_staged(lambda k, w: lend(k, w).start())

    def forward(k, w):
        lend(k, w).wait_recv()
        pass_on(k, w).start()

    m_s[...] = jnp.full(m_s.shape, -1e30, f32)
    l_s[...] = jnp.zeros(l_s.shape, f32)
    acc_s[...] = jnp.zeros(acc_s.shape, f32)
    scale = 1.0 / math.sqrt(dh)

    def clear_tail(k):
        lo, wide = pieces[k][1], cap - pieces[k][1]
        if wide:
            wg[:, lo:] = jnp.zeros((D, wide), bf16)
            wu[:, lo:] = jnp.zeros((D, wide), bf16)
            wd[lo:, :] = jnp.zeros((wide, D), bf16)

    as_hub(clear_tail)

    def attend(yy, blk):
        row_at = (z * 2 + yy) * rows + lax.broadcasted_iota(jnp.int32, (rows, rows), 0)
        col_at = blk * rows + lax.broadcasted_iota(jnp.int32, (rows, rows), 1)
        keep = col_at <= row_at
        for h in range(hh):
            v = kv[blk, :, kw + h * dv : kw + (h + 1) * dv]
            for c in range(2):
                i = 2 * h + c
                k = kv[blk, :, i * dh : (i + 1) * dh]
                s = lax.dot_general(
                    q[yy, :, i * dh : (i + 1) * dh], k, (((1,), (1,)), ((), ())),
                    preferred_element_type=f32,
                ) * scale
                s = jnp.where(keep, s, -1e30)
                old = m_s[yy, i]
                new = jnp.maximum(old, jnp.max(s, axis=1, keepdims=True))
                e = jnp.where(keep, jnp.exp(s - new), 0.0)
                fade = jnp.exp(old - new)
                m_s[yy, i] = new
                l_s[yy, i] = l_s[yy, i] * fade + jnp.sum(e, axis=1, keepdims=True)
                acc_s[yy, i] = acc_s[yy, i] * fade + jnp.dot(
                    e.astype(bf16), v, preferred_element_type=f32
                )

    def late(h):
        return (zi == 0) & (h > z + 1)

    def relay_from(zz, w):
        def go(k):
            @pl.when((zz != z) & jnp.logical_not(staged(zz, k, w)))
            def _():
                with scope("rly"):
                    relay(zz, k, w).wait_recv()
                relay(zz, k, w).start()

        as_hub(go)

    with scope("kvgot"):
        kv_got.wait_recv()
        send_up(mate)
        q_got.wait_recv()

    @pl.loop(0, Z)
    def _(r):
        @pl.when(z >= r)
        def _():
            @pl.when(r > 0)
            def _():
                for blk in (sp - 2 * r, mate - 2 * r):
                    with scope("arrkv"):
                        climb(blk).wait_recv()
                    send_up(blk)

            @pl.loop(0, 4)
            def _(i):
                yy, c = lax.div(i, 2), lax.rem(i, 2)
                with scope("attend"):
                    pl.when((r > 0) | (yy >= c))(lambda: attend(yy, (z - r) * 2 + c))

            @pl.when((r == 1) & (zi == HUBS[1]))
            def _():
                relay_from(z - 1, 0)
                relay_from(z + 1, 1)

            @pl.when((r == 2) & (zi == 3))
            def _():
                forward(1, 0)
                forward(0, 0)

            pl.when((r == 3) & (zi == 3))(lambda: forward(0, 1))

    for i in range(len(targets)):
        h = targets[i][0]
        pl.when((z < h) & jnp.logical_not(early(h) | late(h)))(lambda: direct(i, 0).start())
        pl.when((z < h) & jnp.logical_not(late(h)))(lambda: direct(i, 1).start())

    with scope("nnorm"):
        for yy in range(2):
            for h in range(hh):
                a0 = acc_s[yy, 2 * h] / l_s[yy, 2 * h]
                a1 = acc_s[yy, 2 * h + 1] / l_s[yy, 2 * h + 1]
                a = a0 - lam_ref[y * hh + h] * a1
                ms = jnp.mean(a * a, axis=1, keepdims=True)
                n = a * lax.rsqrt(ms + epsilon) * sub_ref[...] * (1.0 - lambda_init)
                n_own[yy, :, h * dv : (h + 1) * dv] = n.astype(bf16)
    n_swap = pair(n_own.at[other], n_in, 2)
    n_swap.start()
    with scope("relay1"):
        pl.when(zi == HUBS[0])(lambda: relay_from(z + 1, 0))
    with scope("nswapw"):
        loads[3].wait()
        n_swap.wait_recv()
    width = min(512, D)
    hw = hh * dv
    with scope("outproj"):
        for c in range(0, D, width):
            at = slice(c, c + width)
            part[:, :, at] = (
                (
                    jnp.dot(n_own[y], wout[pl.ds(y * hw, hw), at], preferred_element_type=f32)
                    + jnp.dot(n_in[...], wout[pl.ds(other * hw, hw), at], preferred_element_type=f32)
                )
                .astype(bf16)
                .reshape(T, own, width)
            )

    def swap(d):
        return remote(part.at[peer(d)], part_in.at[d], tp_send.at[d], tp_recv.at[d], (sp, peer(d)))

    firsts = [swap(d) for d in range(1, T)]
    for c in firsts:
        c.start()
    twin = jnp.where(zi == HUBS[0], z + 1, z - 1)
    with scope("relayt"):
        pl.when(hub)(lambda: relay_from(twin, 1))
    with scope("rs1"):
        loads[4].wait()
        total = res[...].astype(f32) + part[tp].astype(f32)
        for d in range(1, T):
            firsts[d - 1].wait_recv()
            total = total + part_in[d].astype(f32)
        mid[...] = total
        ms = jnp.mean(total * total, axis=1, keepdims=True)

    def slot(p, t):
        return hn.at[p, pl.ds(pl.multiple_of(t * own, own), own)]

    hn[zi, pl.ds(pl.multiple_of(tp * own, own), own), :] = (
        total * lax.rsqrt(ms + epsilon) * norm_ref[...]
    ).astype(bf16)

    def deliver(k):
        return remote(
            slot(zi, tp), slot(zi, tp), hn_send.at[k], hn_recv.at[zi], ((base + HUBS[k]) * 2 + y, tp)
        )

    pl.when(zi != HUBS[0])(lambda: deliver(0).start())
    pl.when(zi != HUBS[1])(lambda: deliver(1).start())
    for i in range(len(targets)):
        pl.when((z < targets[i][0]) & late(targets[i][0]))(functools.partial(direct_send, i))

    def spread(p, hop):
        src = (tp, tp, far_mate)[hop]
        to = (far_mate, core_mate, core_mate)[hop]
        return remote(slot(p, src), slot(p, src), ag_send.at[p, hop], ag_recv.at[p, hop], (sp, to))

    def gather1(p):
        @pl.when(p != zi)
        def _():
            remote(slot(p, tp), slot(p, tp), hn_send.at[0], hn_recv.at[p], (sp, tp)).wait_recv()

        spread(p, 0).start()
        spread(p, 1).start()

    def gather2(p):
        spread(p, 0).wait_recv()
        spread(p, 2).start()

    @pl.when(hub)
    def _():
        with scope("g1"):
            gather1(zi)

    with scope("relay2"):
        @pl.when(hub)
        def _():
            for w in range(2):
                @pl.loop(0, Z)
                def _(i):
                    done_before = (Z - 1 - i == twin) | ((zi == HUBS[1]) & (Z - 1 - i == z + 1))
                    pl.when(jnp.logical_not(done_before))(lambda: relay_from(Z - 1 - i, w))

    def halo_copy(p):
        last = (y == 1) & (p == GROUP - 1)
        to = jnp.where(last, sp + 2 * GROUP - 1, mate)
        nxt = jnp.where(last, 0, p + y)
        return remote(
            halo_out.at[p], halo_in.at[nxt], halo_send.at[p], halo_recv.at[nxt], (to, tp)
        )

    def halo_sends(p):
        return (y == 0) | (p < GROUP - 1) | (z + GROUP < Z)

    side = D // SPLIT

    def span(h):
        return pl.ds(h * side, side)

    def core_copy(p, i, h):
        return remote(
            low.at[p, (core_mate, diagonal)[i], :, span(h)], low_in.at[p, i, :, span(h)],
            core_send.at[p, i, h], core_recv.at[p, i, h], (sp, core_mate),
        )

    def far_copy(p, h):
        return remote(
            half.at[p, :, span(h)], half_in.at[p, :, span(h)], far_send.at[p, h], far_recv.at[p, h],
            (sp, far_mate),
        )

    def give_back(p, k, h):
        return remote(
            done.at[p, :, span(h)], ret.at[k, :, span(h)], ret_send.at[p, h], ret_recv.at[k, h],
            ((base + p) * 2 + y, tp),
        )

    def reduce1(p, h):
        core_copy(p, 1, h).wait_recv()
        at = slice(h * side, (h + 1) * side)
        half[p, :, at] = (low[p, far_mate, :, at].astype(f32) + low_in[p, 1, :, at].astype(f32)).astype(bf16)
        far_copy(p, h).start()

    def reduce2(p, h):
        core_copy(p, 0, h).wait_recv()
        far_copy(p, h).wait_recv()
        at = slice(h * side, (h + 1) * side)
        t = low[p, tp, :, at].astype(f32) + low_in[p, 0, :, at].astype(f32) + half_in[p, :, at].astype(f32)

        def hand(k):
            @pl.when(p == zi)
            def _():
                ret[k, :, at] = t.astype(bf16)

            @pl.when(p != zi)
            def _():
                done[p, :, at] = t.astype(bf16)
                give_back(p, k, h).start()

        as_hub(hand)

    def feed(p):
        wide = 256
        for c in range(0, cap, wide):
            at = slice(c, c + wide)
            g_s[HALO:, at] = jnp.dot(hn[p], wg[:, at], preferred_element_type=f32).astype(bf16).astype(f32)
            u_s[HALO:, at] = jnp.dot(hn[p], wu[:, at], preferred_element_type=f32).astype(bf16).astype(f32)
        halo_out[p, 0] = g_s[rows:, :].astype(bf16)
        halo_out[p, 1] = u_s[rows:, :].astype(bf16)
        pl.when(halo_sends(p))(lambda: halo_copy(p).start())

        @pl.when(p > 0)
        def _():
            for h in range(SPLIT):
                reduce1(p - 1, h)

        first = (y == 0) & (p == 0) & (base == 0)

        @pl.when(first)
        def _():
            g_s[:HALO, :] = jnp.zeros((HALO, cap), f32)
            u_s[:HALO, :] = jnp.zeros((HALO, cap), f32)

        @pl.when(jnp.logical_not(first))
        def _():
            remote(halo_out.at[p], halo_in.at[p], halo_send.at[p], halo_recv.at[p], (mate, tp)).wait_recv()
            g_s[:HALO, :] = halo_in[p, 0].astype(f32)
            u_s[:HALO, :] = halo_in[p, 1].astype(f32)

        lo = jnp.where(zi == HUBS[0], pieces[0][0], pieces[1][0])
        for c in range(0, cap, LANES):
            at = slice(c, c + LANES)
            tap = pl.ds(pl.multiple_of(jnp.minimum(lo + c, units - LANES), LANES), LANES)

            def mix(x, taps):
                out = taps[0:1, tap] * x[HALO - 2 : HALO - 2 + rows, at]
                out = out + taps[1:2, tap] * x[HALO - 1 : HALO - 1 + rows, at]
                return out + taps[2:3, tap] * x[HALO:, at]

            gm, um = mix(g_s, cg_ref), mix(u_s, cu_ref)
            hid[:, at] = (gm / (1.0 + jnp.exp(-gm)) * um).astype(bf16)
        for c in range(0, D, width):
            at = slice(c, c + width)
            low[p, :, :, at] = (
                jnp.dot(hid[...], wd[:, at], preferred_element_type=f32).astype(bf16).reshape(T, own, width)
            )
            if (c + width) % side == 0:
                core_copy(p, 1, c // side).start()
                core_copy(p, 0, c // side).start()

    def wait_pieces(k):
        for w in range(2):
            own_piece(k, w).wait()

            def arrived(b):
              with scope("arrw"):
                remote(
                    stores[w].at[block(b, k)], stores[w].at[block(b, k)],
                    cross_send.at[w], w_recv.at[w, b], (mate, tp),
                ).wait_recv()

            @pl.loop(0, Z)
            def _(zz):
                pl.when(staged(zz, k, w))(lambda: arrived(zz * 2 + y))
                arrived(zz * 2 + other)

        down_piece(k).wait()

    @pl.when(hub)
    def _():
        with scope("ga"):
            pl.when(zi != HUBS[0])(lambda: gather1(HUBS[0]))
            gather1(0)
            gather2(zi)
            pl.when(zi != HUBS[0])(lambda: gather2(HUBS[0]))
            pl.when(zi != HUBS[1])(lambda: gather1(HUBS[1]))
            gather2(0)

        with scope("wwait"):
            as_hub(wait_pieces)

        @pl.loop(0, GROUP)
        def _(p):
            @pl.when(p == 0)
            def _():
                with scope("gather2"):
                    gather1(GROUP - 1)

            @pl.when(p == 1)
            def _():
                with scope("gather3"):
                    pl.when(zi != HUBS[1])(lambda: gather2(HUBS[1]))

            @pl.when(p == 2)
            def _():
                with scope("gather4"):
                    gather2(GROUP - 1)

            with scope("agw"):
                spread(p, 1).wait_recv()
                spread(p, 2).wait_recv()
            with scope("feed"):
                feed(p)

        with scope("redlast"):
            for h in range(SPLIT):
                with scope("r13"):
                    reduce1(GROUP - 1, h)
            for p in range(GROUP):
                for h in range(SPLIT):
                    with scope(f"r2{p}{h}"):
                        reduce2(p, h)

    with scope("final"):
        for h in range(SPLIT):
            at = slice(h * side, (h + 1) * side)
            total = mid[:, at]
            for k in range(2):
                got = remote(
                    done.at[0, :, span(h)], ret.at[k, :, span(h)], ret_send.at[0, h], ret_recv.at[k, h], (sp, tp)
                )
                pl.when(zi != HUBS[k])(got.wait_recv)
                total = total + ret[k, :, at].astype(f32)
            out_ref[:, at] = total.astype(bf16)

    with scope("drain"):
        @pl.loop(0, Z)
        def _(zz):
            @pl.when(has_up & (zz <= z))
            def _():
                climb(2 * zz).wait_send()
                climb(2 * zz + 1).wait_send()

            def go(k):
                for w in range(2):
                    pl.when((zz != z) & jnp.logical_not(staged(zz, k, w)))(relay(zz, k, w).wait_send)

            as_hub(go)

        for i in range(len(targets)):
            @pl.when(z != targets[i][0])
            def _():
                direct(i, 0).wait_send()
                direct(i, 1).wait_send()

        def cross_end(k):
            cross(k, 0).wait_send()
            cross(k, 1).wait_send()

        as_hub(cross_end)

        def lend_end(k, w):
            lend(k, w).wait_send()
            pass_on(k, w).wait_send()

        each_staged(lend_end)
        for c in firsts + [kv_swap, q_swap, n_swap]:
            c.wait_send()
        for k in range(2):
            pl.when(zi != HUBS[k])(lambda: deliver(k).wait_send())

        @pl.when(hub)
        def _():
            @pl.loop(0, GROUP)
            def _(p):
                for hop in range(3):
                    spread(p, hop).wait_send()
                pl.when(halo_sends(p))(lambda: halo_copy(p).wait_send())
                for h in range(SPLIT):
                    core_copy(p, 0, h).wait_send()
                    core_copy(p, 1, h).wait_send()
                    far_copy(p, h).wait_send()
                    pl.when(p != zi)(give_back(p, 0, h).wait_send)


def local(
    S, T,
    residual, queries, key_rows, values, lambda_head, sub_gain, w_out, norm_gain,
    w_gate, w_up, conv_gate, conv_up, w_down,
):
    rows, heads, maps, dh = queries.shape
    dv = values.shape[2]
    feat, units = w_gate.shape
    D = w_out.shape[1]
    own = rows // T
    cap = max(p[1] for p in parts_of(units))
    hh = heads // 2
    qw = hh * maps * dh
    kvw = qw + hh * dv
    Z = S // 2
    hbm = pl.BlockSpec(memory_space=pl.ANY)
    vmem = pl.BlockSpec(memory_space=pltpu.VMEM)
    smem = pl.BlockSpec(memory_space=pltpu.SMEM)
    V = pltpu.VMEM
    dma = pltpu.SemaphoreType.DMA
    return pl.pallas_call(
        functools.partial(kernel, S, T, heads, dh, dv),
        out_shape=jax.ShapeDtypeStruct((own, D), bf16),
        in_specs=[hbm] * 8 + [smem] + [vmem] * 4,
        out_specs=vmem,
        scratch_shapes=[
            V(queries.shape, bf16),
            V(key_rows.shape, bf16),
            V(values.shape, bf16),
            V((rows, qw), bf16),
            V((rows, kvw), bf16),
            V((2, rows, qw), bf16),
            V((S, rows, kvw), bf16),
            V((own, D), bf16),
            V(w_out.shape, bf16),
            V((D, cap), bf16),
            V((D, cap), bf16),
            V((cap, D), bf16),
            V((2, 2, feat, cap), bf16),
            V((2, 2 * hh, rows, 1), f32),
            V((2, 2 * hh, rows, 1), f32),
            V((2, 2 * hh, rows, dv), f32),
            V((2, rows, hh * dv), bf16),
            V((rows, hh * dv), bf16),
            V((T, own, D), bf16),
            V((T, own, D), bf16),
            V((own, D), f32),
            V((GROUP, rows, D), bf16),
            V((rows + HALO, cap), f32),
            V((rows + HALO, cap), f32),
            V((GROUP, 2, HALO, cap), bf16),
            V((GROUP, 2, HALO, cap), bf16),
            V((rows, cap), bf16),
            V((GROUP, T, own, D), bf16),
            V((GROUP, 2, own, D), bf16),
            V((GROUP, own, D), bf16),
            V((GROUP, own, D), bf16),
            V((GROUP, own, D), bf16),
            V((2, own, D), bf16),
            dma((5,)),
            dma((3,)),
            dma((2, 3)),
            dma((S,)),
            dma((S,)),
            dma((2, Z // 2)),
            dma((2, S)),
            dma((2,)),
            dma((2, 2)),
            dma((2, 2)),
            dma((2, 2)),
            dma((2, Z)),
            dma((T,)),
            dma((T,)),
            dma((2,)),
            dma((GROUP,)),
            dma((GROUP, 3)),
            dma((GROUP, 3)),
            dma((GROUP,)),
            dma((GROUP,)),
            dma((GROUP, 2, SPLIT)),
            dma((GROUP, 2, SPLIT)),
            dma((GROUP, SPLIT)),
            dma((GROUP, SPLIT)),
            dma((GROUP, SPLIT)),
            dma((2, SPLIT)),
        ],
        compiler_params=pltpu.CompilerParams(
            collective_id=0, has_side_effects=True, vmem_limit_bytes=64000000
        ),
    )(
        queries, key_rows, values, residual, w_out, w_gate, w_up, w_down, lambda_head,
        sub_gain.reshape(1, -1), norm_gain.reshape(1, -1), conv_gate, conv_up,
    )


def solution(mesh):
    placed = (
        P("sp", None),
        P("sp", "tp", None, None),
        P("sp", "tp", None, None),
        P("sp", "tp", None),
        P("tp"),
        P(),
        P("tp", None),
        P(),
        P("sp", "tp"),
        P("sp", "tp"),
        P(None, "tp"),
        P(None, "tp"),
        P("tp", None),
    )
    return jax.shard_map(
        functools.partial(local, mesh.shape["sp"], mesh.shape["tp"]),
        mesh=mesh, in_specs=placed, out_specs=P(("sp", "tp"), None), check_vma=False,
    )
```

```python
import contextlib
import functools
import math

import jax
import jax.numpy as jnp
from jax import lax
from jax.experimental import pallas as pl
from jax.experimental.pallas import tpu as pltpu
from jax.sharding import PartitionSpec as P

MESH = pl.DeviceIdType.MESH
epsilon = 1e-06
lambda_init = 0.8 - 0.6 * math.exp(-0.3)
bf16 = jnp.bfloat16
f32 = jnp.float32
HALO = 16
GROUP = 4
HUBS = (1, 2)
LANES = 128
SPLIT = 2
STAGED = {3: ((0, 0), (1, 0), (0, 1))}


def scope(name):
    return contextlib.nullcontext()


def parts_of(units):
    chunks = units // LANES
    first = (chunks + 1) // 2
    return ((0, first * LANES), (first * LANES, (chunks - first) * LANES))


def kernel(
    S, T, heads, dh, dv,
    q_hbm, k_hbm, v_hbm, res_hbm, wout_hbm, wg_hbm, wu_hbm, wd_hbm,
    lam_ref, sub_ref, norm_ref, cg_ref, cu_ref,
    out_ref,
    q_raw, k_raw, v_raw, q_out, kv_out, q, kv, res, wout, wg, wu, wd, stage,
    m_s, l_s, acc_s, n_own, n_in, part, part_in, mid, hn,
    g_s, u_s, halo_out, halo_in, hid, low, low_in, half, half_in, done, ret, home_out, home_in,
    local_sem, own_sem, pair_sem, kv_send, kv_recv,
    w_send, w_recv, cross_send, lend_send, stage_recv, stage_send, relay_send,
    tp_send, tp_recv, hn_send, hn_recv, ag_send, ag_recv,
    halo_send, halo_recv, core_send, core_recv, far_send, far_recv, ret_send, ret_recv, home_send, home_recv, go_sem,
):
    Z = S // 2
    sp = lax.axis_index("sp")
    tp = lax.axis_index("tp")
    z = lax.div(sp, 2)
    y = lax.rem(sp, 2)
    zi = lax.rem(z, GROUP)
    base = z - zi
    rows = q.shape[1]
    feat, units = wg_hbm.shape
    hh = heads // 2
    kw = 2 * hh * dh
    D = wout.shape[1]
    own = rows // T
    cap = wg.shape[1]
    pieces = parts_of(units)
    other = 1 - y
    mate = z * 2 + other
    has_up = z < Z - 1
    hub = (zi == HUBS[0]) | (zi == HUBS[1])
    core_mate = tp + 1 - 2 * lax.rem(tp, 2)
    far_mate = lax.rem(tp + 2, T)
    diagonal = T - 1 - tp

    def one(flag):
        return flag.astype(jnp.int32)

    def peer(d):
        return lax.rem(tp + d, T)

    def remote(src, dst, send, recv, device):
        return pltpu.make_async_remote_copy(
            src_ref=src, dst_ref=dst, send_sem=send, recv_sem=recv, device_id=device, device_id_type=MESH
        )

    def cols(k):
        return pl.ds(pieces[k][0], pieces[k][1])

    def block(b, k):
        return (pl.ds(pl.multiple_of(b * feat, feat), feat), pl.ds(0, pieces[k][1]))

    sources, stores = (wg_hbm, wu_hbm), (wg, wu)
    targets = [(g * GROUP + HUBS[k], k) for g in range(Z // GROUP) for k in range(2)]

    def direct(i, w):
        h, k = targets[i]
        return remote(
            sources[w].at[:, cols(k)], stores[w].at[block(sp, k)],
            w_send.at[w, i], w_recv.at[w, sp], (h * 2 + y, tp),
        )

    def cross(k, w):
        return remote(
            sources[w].at[:, cols(k)], stores[w].at[block(sp, k)],
            cross_send.at[w], w_recv.at[w, sp], (mate, tp),
        )

    def lend(k, w):
        return remote(
            sources[w].at[:, cols(k)], stage.at[k, w, :, pl.ds(0, pieces[k][1])],
            lend_send.at[k, w], stage_recv.at[k, w], (mate, tp),
        )

    def pass_on(k, w):
        h = base + HUBS[k]
        return remote(
            stage.at[k, w, :, pl.ds(0, pieces[k][1])], stores[w].at[block(mate, k)],
            stage_send.at[k, w], w_recv.at[w, mate], (h * 2 + y, tp),
        )

    def staged(zz, k, w):
        hit = zz < 0
        for zo, which in STAGED.items():
            if (k, w) in which:
                hit = hit | (zz == base + zo)
        return hit

    def each_staged(fn):
        for zo, which in STAGED.items():
            for k, w in which:
                pl.when(zi == zo)(functools.partial(fn, k, w))

    def relay(zz, k, w):
        b = zz * 2 + y
        return remote(
            stores[w].at[block(b, k)], stores[w].at[block(b, k)],
            relay_send.at[w, zz], w_recv.at[w, b], (mate, tp),
        )

    def own_piece(k, w):
        return pltpu.make_async_copy(sources[w].at[:, cols(k)], stores[w].at[block(sp, k)], own_sem.at[w])

    def down_piece(k):
        return pltpu.make_async_copy(
            wd_hbm.at[cols(k), :], wd.at[pl.ds(0, pieces[k][1]), :], own_sem.at[2]
        )

    def as_hub(fn):
        for k in range(2):
            pl.when(zi == HUBS[k])(functools.partial(fn, k))

    loads = [
        pltpu.make_async_copy(k_hbm, k_raw, local_sem.at[0]),
        pltpu.make_async_copy(v_hbm, v_raw, local_sem.at[4]),
        pltpu.make_async_copy(q_hbm, q_raw, local_sem.at[1]),
        pltpu.make_async_copy(wout_hbm, wout, local_sem.at[2]),
        pltpu.make_async_copy(res_hbm.at[pl.ds(pl.multiple_of(tp * own, own), own), :], res, local_sem.at[3]),
    ]
    for c in loads:
        c.start()

    def load_pieces(k):
        own_piece(k, 0).start()
        own_piece(k, 1).start()
        down_piece(k).start()

    as_hub(load_pieces)

    barrier = pltpu.get_barrier_semaphore()
    next_group, prev_group = (y == 1) & (z + GROUP < Z), (y == 0) & (z >= GROUP)

    def greet(device):
        pl.semaphore_signal(barrier, inc=1, device_id=device, device_id_type=MESH)

    with scope("barrier"):
        for zz in range(Z):
            pl.when(z != zz)(functools.partial(greet, (zz * 2 + y, tp)))
        greet((mate, tp))
        for d in range(1, T):
            greet((sp, peer(d)))
        pl.when(next_group)(lambda: greet((sp + 2 * GROUP - 1, tp)))
        pl.when(prev_group)(lambda: greet((sp - 2 * GROUP + 1, tp)))
        with scope("relayout"):
            for c in loads[:3]:
                c.wait()
            for yy in range(2):
                @pl.when(y == yy)
                def _():
                    for mine, q_to, kv_to in ((True, q.at[y], kv.at[sp]), (False, q_out, kv_out)):
                        for h in range(hh):
                            head = (yy if mine else 1 - yy) * hh + h
                            for c in range(2):
                                i = 2 * h + c
                                q_to[:, i * dh : (i + 1) * dh] = q_raw[:, head, c, :]
                                kv_to[:, i * dh : (i + 1) * dh] = k_raw[:, head, c, :]
                            kv_to[:, kw + h * dv : kw + (h + 1) * dv] = v_raw[:, head, :]
        pl.semaphore_wait(barrier, Z + T - 1 + one(next_group) + one(prev_group))

    def climb(blk):
        return remote(kv.at[blk], kv.at[blk], kv_send.at[blk], kv_recv.at[blk], (sp + 2, tp))

    def send_up(blk):
        pl.when(has_up)(lambda: climb(blk).start())

    def pair(src, dst, k):
        return remote(src, dst, pair_sem.at[0, k], pair_sem.at[1, k], (mate, tp))

    kv_swap = pair(kv_out, kv.at[sp], 0)
    q_swap = pair(q_out, q.at[y], 1)
    kv_got = pair(kv_out, kv.at[mate], 0)
    q_got = pair(q_out, q.at[other], 1)
    kv_swap.start()
    q_swap.start()
    send_up(sp)

    def direct_send(i):
        direct(i, 0).start()
        direct(i, 1).start()

    def second(h):
        return (zi == 3) & (h == z - 2)

    for i in reversed(range(len(targets))):
        h = targets[i][0]
        pl.when((z > h) & jnp.logical_not(second(h)))(functools.partial(direct_send, i))

    def cross_start(k):
        cross(k, 0).start()
        if k == 1:
            cross(k, 1).start()

    as_hub(cross_start)
    each_staged(lambda k, w: lend(k, w).start())

    def forward(k, w):
        lend(k, w).wait_recv()
        pass_on(k, w).start()

    m_s[...] = jnp.full(m_s.shape, -1e30, f32)
    l_s[...] = jnp.zeros(l_s.shape, f32)
    acc_s[...] = jnp.zeros(acc_s.shape, f32)
    scale = 1.0 / math.sqrt(dh)

    def clear_tail(k):
        lo, wide = pieces[k][1], cap - pieces[k][1]
        if wide:
            wg[:, lo:] = jnp.zeros((D, wide), bf16)
            wu[:, lo:] = jnp.zeros((D, wide), bf16)
            wd[lo:, :] = jnp.zeros((wide, D), bf16)

    as_hub(clear_tail)

    def attend(yy, blk):
        row_at = (z * 2 + yy) * rows + lax.broadcasted_iota(jnp.int32, (rows, rows), 0)
        col_at = blk * rows + lax.broadcasted_iota(jnp.int32, (rows, rows), 1)
        keep = col_at <= row_at
        for h in range(hh):
            v = kv[blk, :, kw + h * dv : kw + (h + 1) * dv]
            for c in range(2):
                i = 2 * h + c
                k = kv[blk, :, i * dh : (i + 1) * dh]
                s = lax.dot_general(
                    q[yy, :, i * dh : (i + 1) * dh], k, (((1,), (1,)), ((), ())),
                    preferred_element_type=f32,
                ) * scale
                s = jnp.where(keep, s, -1e30)
                old = m_s[yy, i]
                new = jnp.maximum(old, jnp.max(s, axis=1, keepdims=True))
                e = jnp.where(keep, jnp.exp(s - new), 0.0)
                fade = jnp.exp(old - new)
                m_s[yy, i] = new
                l_s[yy, i] = l_s[yy, i] * fade + jnp.sum(e, axis=1, keepdims=True)
                acc_s[yy, i] = acc_s[yy, i] * fade + jnp.dot(
                    e.astype(bf16), v, preferred_element_type=f32
                )

    def late(h):
        return (zi == 0) & (h > z + 1)

    def relay_from(zz, w):
        def go(k):
            @pl.when((zz != z) & jnp.logical_not(staged(zz, k, w)))
            def _():
                with scope("rly"):
                    relay(zz, k, w).wait_recv()
                relay(zz, k, w).start()

        as_hub(go)

    with scope("kvgot"):
        kv_got.wait_recv()
        send_up(mate)
        q_got.wait_recv()

    @pl.loop(0, Z)
    def _(r):
        @pl.when(z >= r)
        def _():
            @pl.when(r > 0)
            def _():
                for blk in (sp - 2 * r, mate - 2 * r):
                    with scope("arrkv"):
                        climb(blk).wait_recv()
                    send_up(blk)

            @pl.loop(0, 4)
            def _(i):
                yy, c = lax.div(i, 2), lax.rem(i, 2)
                with scope("attend"):
                    pl.when((r > 0) | (yy >= c))(lambda: attend(yy, (z - r) * 2 + c))

            @pl.when((r == 1) & (zi == HUBS[1]))
            def _():
                relay_from(z + 1, 1)

            @pl.when((r == 2) & (zi == 3))
            def _():
                forward(0, 0)

            @pl.when((r == 3) & (zi == 3))
            def _():
                forward(1, 0)
                forward(0, 1)

            for i in range(len(targets)):
                pl.when((r == 1) & second(targets[i][0]))(functools.partial(direct_send, i))

    for i in range(len(targets)):
        h = targets[i][0]
        pl.when((z < h) & jnp.logical_not(late(h)))(functools.partial(direct_send, i))

    with scope("nnorm"):
        for yy in range(2):
            for h in range(hh):
                a0 = acc_s[yy, 2 * h] / l_s[yy, 2 * h]
                a1 = acc_s[yy, 2 * h + 1] / l_s[yy, 2 * h + 1]
                a = a0 - lam_ref[y * hh + h] * a1
                ms = jnp.mean(a * a, axis=1, keepdims=True)
                n = a * lax.rsqrt(ms + epsilon) * sub_ref[...] * (1.0 - lambda_init)
                n_own[yy, :, h * dv : (h + 1) * dv] = n.astype(bf16)
    n_swap = pair(n_own.at[other], n_in, 2)
    n_swap.start()
    with scope("relay1"):
        @pl.when(zi == HUBS[0])
        def _():
            relay_from(z + 1, 0)
            cross(0, 1).start()

    with scope("nswapw"):
        loads[3].wait()
        n_swap.wait_recv()
    width = min(512, D)
    hw = hh * dv
    with scope("outproj"):
        for c in range(0, D, width):
            at = slice(c, c + width)
            part[:, :, at] = (
                (
                    jnp.dot(n_own[y], wout[pl.ds(y * hw, hw), at], preferred_element_type=f32)
                    + jnp.dot(n_in[...], wout[pl.ds(other * hw, hw), at], preferred_element_type=f32)
                )
                .astype(bf16)
                .reshape(T, own, width)
            )

    def swap(d):
        return remote(part.at[peer(d)], part_in.at[d], tp_send.at[d], tp_recv.at[d], (sp, peer(d)))

    firsts = [swap(d) for d in range(1, T)]
    for c in firsts:
        c.start()
    twin = jnp.where(zi == HUBS[0], z + 1, z - 1)
    with scope("relayt"):
        pl.when(zi == HUBS[1])(lambda: relay_from(twin, 0))
    with scope("rs1"):
        loads[4].wait()
        total = res[...].astype(f32) + part[tp].astype(f32)
        for d in range(1, T):
            firsts[d - 1].wait_recv()
            total = total + part_in[d].astype(f32)
        mid[...] = total
        ms = jnp.mean(total * total, axis=1, keepdims=True)

    def slot(p, t):
        return hn.at[p, pl.ds(pl.multiple_of(t * own, own), own)]

    hn[zi, pl.ds(pl.multiple_of(tp * own, own), own), :] = (
        total * lax.rsqrt(ms + epsilon) * norm_ref[...]
    ).astype(bf16)

    def deliver(k):
        return remote(
            slot(zi, tp), slot(zi, tp), hn_send.at[k], hn_recv.at[zi], ((base + HUBS[k]) * 2 + y, tp)
        )

    pl.when(zi != HUBS[0])(lambda: deliver(0).start())
    pl.when((zi == 0) | (zi == 3))(lambda: deliver(1).start())

    @pl.when(zi == 0)
    def _():
        pl.semaphore_wait(go_sem, 1)
        for i in range(len(targets)):
            pl.when(late(targets[i][0]))(functools.partial(direct_send, i))


    def spread(p, hop):
        src = (tp, tp, far_mate)[hop]
        to = (far_mate, core_mate, core_mate)[hop]
        return remote(slot(p, src), slot(p, src), ag_send.at[p, hop], ag_recv.at[p, hop], (sp, to))

    def gather1(p):
        @pl.when(p != zi)
        def _():
            remote(slot(p, tp), slot(p, tp), hn_send.at[0], hn_recv.at[p], (sp, tp)).wait_recv()

        spread(p, 0).start()
        spread(p, 1).start()

    def gather2(p):
        spread(p, 0).wait_recv()
        spread(p, 2).start()

    @pl.when(hub)
    def _():
        with scope("g1"):
            gather1(zi)

    with scope("relay2"):
        @pl.when(hub)
        def _():
            gather1(0)
            relay_from(twin, 1)
            for w in range(2):
                @pl.loop(0, Z)
                def _(i):
                    done_before = (Z - 1 - i == twin) | ((zi == HUBS[1]) & (Z - 1 - i == z + 1))
                    pl.when(jnp.logical_not(done_before))(lambda: relay_from(Z - 1 - i, w))

    def halo_copy(p):
        last = (y == 1) & (p == GROUP - 1)
        to = jnp.where(last, sp + 2 * GROUP - 1, mate)
        nxt = jnp.where(last, 0, p + y)
        return remote(
            halo_out.at[p], halo_in.at[nxt], halo_send.at[p], halo_recv.at[nxt], (to, tp)
        )

    def halo_sends(p):
        return (y == 0) | (p < GROUP - 1) | (z + GROUP < Z)

    side = D // SPLIT

    def span(h):
        return pl.ds(h * side, side)

    def core_copy(p, i, h):
        return remote(
            low.at[p, (core_mate, diagonal)[i], :, span(h)], low_in.at[p, i, :, span(h)],
            core_send.at[p, i, h], core_recv.at[p, i, h], (sp, core_mate),
        )

    def far_copy(p, h):
        return remote(
            half.at[p, :, span(h)], half_in.at[p, :, span(h)], far_send.at[p, h], far_recv.at[p, h],
            (sp, far_mate),
        )

    def give_back(p, k, h):
        return remote(
            done.at[p, :, span(h)], ret.at[k, :, span(h)], ret_send.at[p, h], ret_recv.at[k, h],
            ((base + p) * 2 + y, tp),
        )

    def reduce1(p, h):
        core_copy(p, 1, h).wait_recv()
        at = slice(h * side, (h + 1) * side)
        half[p, :, at] = (low[p, far_mate, :, at].astype(f32) + low_in[p, 1, :, at].astype(f32)).astype(bf16)
        far_copy(p, h).start()

    def home_copy(k, i, h):
        return remote(
            home_out.at[i, :, span(h)], home_in.at[k, i, :, span(h)],
            home_send.at[i, h], home_recv.at[k, i, h], (base * 2 + y, tp),
        )

    def send_home(h):
        at = slice(h * side, (h + 1) * side)
        for i, t in ((1, far_mate), (0, tp)):
            core_copy(0, i, h).wait_recv()
            home_out[i, :, at] = (low[0, t, :, at].astype(f32) + low_in[0, i, :, at].astype(f32)).astype(bf16)
            as_hub(lambda k: home_copy(k, i, h).start())

    def reduce2(p, h):
        core_copy(p, 0, h).wait_recv()
        far_copy(p, h).wait_recv()
        at = slice(h * side, (h + 1) * side)
        t = low[p, tp, :, at].astype(f32) + low_in[p, 0, :, at].astype(f32) + half_in[p, :, at].astype(f32)

        def hand(k):
            @pl.when(p == zi)
            def _():
                ret[k, :, at] = t.astype(bf16)

            @pl.when(p != zi)
            def _():
                done[p, :, at] = t.astype(bf16)
                give_back(p, k, h).start()

        as_hub(hand)

    def feed(p):
        wide = 256
        for c in range(0, cap, wide):
            at = slice(c, c + wide)
            g_s[HALO:, at] = jnp.dot(hn[p], wg[:, at], preferred_element_type=f32).astype(bf16).astype(f32)
            u_s[HALO:, at] = jnp.dot(hn[p], wu[:, at], preferred_element_type=f32).astype(bf16).astype(f32)
        halo_out[p, 0] = g_s[rows:, :].astype(bf16)
        halo_out[p, 1] = u_s[rows:, :].astype(bf16)
        pl.when(halo_sends(p))(lambda: halo_copy(p).start())

        lo = jnp.where(zi == HUBS[0], pieces[0][0], pieces[1][0])

        def conv(start, count):
            for c in range(0, cap, LANES):
                at = slice(c, c + LANES)
                tap = pl.ds(pl.multiple_of(jnp.minimum(lo + c, units - LANES), LANES), LANES)

                def mix(x, taps):
                    at0 = HALO + start
                    out = taps[0:1, tap] * x[at0 - 2 : at0 - 2 + count, at]
                    out = out + taps[1:2, tap] * x[at0 - 1 : at0 - 1 + count, at]
                    return out + taps[2:3, tap] * x[at0 : at0 + count, at]

                gm, um = mix(g_s, cg_ref), mix(u_s, cu_ref)
                hid[start : start + count, at] = (gm / (1.0 + jnp.exp(-gm)) * um).astype(bf16)

        @pl.when(p > 0)
        def _():
            @pl.when(p == 1)
            def _():
                for h in range(SPLIT):
                    send_home(h)

            @pl.when(p > 1)
            def _():
                reduce1(p - 1, 0)
                pl.when(p < GROUP - 1)(lambda: reduce1(p - 1, 1))

        conv(HALO, rows - HALO)
        pl.when(p == GROUP - 2)(lambda: gather2(GROUP - 1))
        first = (y == 0) & (p == 0) & (base == 0)

        @pl.when(first)
        def _():
            g_s[:HALO, :] = jnp.zeros((HALO, cap), f32)
            u_s[:HALO, :] = jnp.zeros((HALO, cap), f32)

        @pl.when(jnp.logical_not(first))
        def _():
            with scope("halo"):
                remote(halo_out.at[p], halo_in.at[p], halo_send.at[p], halo_recv.at[p], (mate, tp)).wait_recv()
            g_s[:HALO, :] = halo_in[p, 0].astype(f32)
            u_s[:HALO, :] = halo_in[p, 1].astype(f32)

        conv(0, HALO)
        for c in range(0, D, width):
            at = slice(c, c + width)
            low[p, :, :, at] = (
                jnp.dot(hid[...], wd[:, at], preferred_element_type=f32).astype(bf16).reshape(T, own, width)
            )
            if (c + width) % side == 0:
                core_copy(p, 1, c // side).start()
                core_copy(p, 0, c // side).start()

    def wait_pieces(k):
        for w in range(2):
            own_piece(k, w).wait()

            def arrived(b):
              with scope("arrw"):
                remote(
                    stores[w].at[block(b, k)], stores[w].at[block(b, k)],
                    cross_send.at[w], w_recv.at[w, b], (mate, tp),
                ).wait_recv()

            @pl.loop(0, Z)
            def _(zz):
                pl.when(staged(zz, k, w))(lambda: arrived(zz * 2 + y))
                arrived(zz * 2 + other)

        down_piece(k).wait()

    with scope("go"):
        @pl.when(zi == HUBS[0])
        def _():
            for i in range(len(targets)):
                @pl.when(targets[i][0] == z + 1)
                def _():
                    direct(i, 0).wait_send()
                    direct(i, 1).wait_send()

            pl.semaphore_signal(go_sem, inc=1, device_id=(sp - 2, tp), device_id_type=MESH)
            deliver(1).start()

    @pl.when(hub)
    def _():
        with scope("ga"):
            gather2(zi)
            gather2(0)
            pl.when(zi == HUBS[0])(lambda: gather1(HUBS[1]))
            pl.when(zi == HUBS[1])(lambda: gather1(HUBS[0]))

        with scope("wwait"):
            as_hub(wait_pieces)

        @pl.loop(0, GROUP)
        def _(p):
            other_hub = jnp.where(zi == HUBS[0], HUBS[1], HUBS[0])
            with scope("gat"):
                pl.when(p == 0)(lambda: gather1(GROUP - 1))
                pl.when(p == other_hub)(lambda: gather2(other_hub))

            with scope("agw"):
                spread(p, 1).wait_recv()
                spread(p, 2).wait_recv()
            with scope("feed"):
                feed(p)

        with scope("redlast"):
            for p, h in ((3, 0), (3, 1), (2, 1)):
                with scope("r1"):
                    reduce1(p, h)
            for p, h in ((1, 0), (1, 1), (2, 0), (3, 0), (3, 1), (2, 1)):
                with scope(f"r2{p}{h}"):
                    reduce2(p, h)

    with scope("final"):
        @pl.when(zi == 0)
        def _():
            for h in range(SPLIT):
                at = slice(h * side, (h + 1) * side)
                for k in range(2):
                    home_copy(k, 1, h).wait_recv()
                half[0, :, at] = (home_in[0, 1, :, at].astype(f32) + home_in[1, 1, :, at].astype(f32)).astype(bf16)
                far_copy(0, h).start()
            for h in range(SPLIT):
                at = slice(h * side, (h + 1) * side)
                for k in range(2):
                    home_copy(k, 0, h).wait_recv()
                total = mid[:, at] + home_in[0, 0, :, at].astype(f32) + home_in[1, 0, :, at].astype(f32)
                far_copy(0, h).wait_recv()
                out_ref[:, at] = (total + half_in[0, :, at].astype(f32)).astype(bf16)

        @pl.when(zi != 0)
        def _():
            for h in range(SPLIT):
                at = slice(h * side, (h + 1) * side)
                total = mid[:, at]
                for k in range(2):
                    got = remote(
                        done.at[0, :, span(h)], ret.at[k, :, span(h)], ret_send.at[0, h], ret_recv.at[k, h], (sp, tp)
                    )
                    pl.when(zi != HUBS[k])(got.wait_recv)
                    total = total + ret[k, :, at].astype(f32)
                out_ref[:, at] = total.astype(bf16)

    with scope("drain"):
        @pl.loop(0, Z)
        def _(zz):
            @pl.when(has_up & (zz <= z))
            def _():
                climb(2 * zz).wait_send()
                climb(2 * zz + 1).wait_send()

            def go(k):
                for w in range(2):
                    pl.when((zz != z) & jnp.logical_not(staged(zz, k, w)))(relay(zz, k, w).wait_send)

            as_hub(go)

        for i in range(len(targets)):
            @pl.when((z != targets[i][0]) & ((zi != HUBS[0]) | (targets[i][0] != z + 1)))
            def _():
                direct(i, 0).wait_send()
                direct(i, 1).wait_send()

        def cross_end(k):
            cross(k, 0).wait_send()
            cross(k, 1).wait_send()

        as_hub(cross_end)

        def lend_end(k, w):
            lend(k, w).wait_send()
            pass_on(k, w).wait_send()

        each_staged(lend_end)
        for c in firsts + [kv_swap, q_swap, n_swap]:
            c.wait_send()
        for k in range(2):
            pl.when(zi != HUBS[k])(lambda: deliver(k).wait_send())

        @pl.when(zi == 0)
        def _():
            for h in range(SPLIT):
                far_copy(0, h).wait_send()

        @pl.when(hub)
        def _():
            for h in range(SPLIT):
                for i in range(2):
                    home_copy(0, i, h).wait_send()

            @pl.loop(0, GROUP)
            def _(p):
                for hop in range(3):
                    spread(p, hop).wait_send()
                pl.when(halo_sends(p))(lambda: halo_copy(p).wait_send())
                for h in range(SPLIT):
                    core_copy(p, 0, h).wait_send()
                    core_copy(p, 1, h).wait_send()
                    pl.when(p > 0)(far_copy(p, h).wait_send)
                    pl.when((p > 0) & (p != zi))(give_back(p, 0, h).wait_send)


def local(
    S, T,
    residual, queries, key_rows, values, lambda_head, sub_gain, w_out, norm_gain,
    w_gate, w_up, conv_gate, conv_up, w_down,
):
    rows, heads, maps, dh = queries.shape
    dv = values.shape[2]
    feat, units = w_gate.shape
    D = w_out.shape[1]
    own = rows // T
    cap = max(p[1] for p in parts_of(units))
    hh = heads // 2
    qw = hh * maps * dh
    kvw = qw + hh * dv
    Z = S // 2
    hbm = pl.BlockSpec(memory_space=pl.ANY)
    vmem = pl.BlockSpec(memory_space=pltpu.VMEM)
    smem = pl.BlockSpec(memory_space=pltpu.SMEM)
    V = pltpu.VMEM
    dma = pltpu.SemaphoreType.DMA
    return pl.pallas_call(
        functools.partial(kernel, S, T, heads, dh, dv),
        out_shape=jax.ShapeDtypeStruct((own, D), bf16),
        in_specs=[hbm] * 8 + [smem] + [vmem] * 4,
        out_specs=vmem,
        scratch_shapes=[
            V(queries.shape, bf16),
            V(key_rows.shape, bf16),
            V(values.shape, bf16),
            V((rows, qw), bf16),
            V((rows, kvw), bf16),
            V((2, rows, qw), bf16),
            V((S, rows, kvw), bf16),
            V((own, D), bf16),
            V(w_out.shape, bf16),
            V((D, cap), bf16),
            V((D, cap), bf16),
            V((cap, D), bf16),
            V((2, 2, feat, cap), bf16),
            V((2, 2 * hh, rows, 1), f32),
            V((2, 2 * hh, rows, 1), f32),
            V((2, 2 * hh, rows, dv), f32),
            V((2, rows, hh * dv), bf16),
            V((rows, hh * dv), bf16),
            V((T, own, D), bf16),
            V((T, own, D), bf16),
            V((own, D), f32),
            V((GROUP, rows, D), bf16),
            V((rows + HALO, cap), f32),
            V((rows + HALO, cap), f32),
            V((GROUP, 2, HALO, cap), bf16),
            V((GROUP, 2, HALO, cap), bf16),
            V((rows, cap), bf16),
            V((GROUP, T, own, D), bf16),
            V((GROUP, 2, own, D), bf16),
            V((GROUP, own, D), bf16),
            V((GROUP, own, D), bf16),
            V((GROUP, own, D), bf16),
            V((2, own, D), bf16),
            V((2, own, D), bf16),
            V((2, 2, own, D), bf16),
            dma((5,)),
            dma((3,)),
            dma((2, 3)),
            dma((S,)),
            dma((S,)),
            dma((2, Z // 2)),
            dma((2, S)),
            dma((2,)),
            dma((2, 2)),
            dma((2, 2)),
            dma((2, 2)),
            dma((2, Z)),
            dma((T,)),
            dma((T,)),
            dma((2,)),
            dma((GROUP,)),
            dma((GROUP, 3)),
            dma((GROUP, 3)),
            dma((GROUP,)),
            dma((GROUP,)),
            dma((GROUP, 2, SPLIT)),
            dma((GROUP, 2, SPLIT)),
            dma((GROUP, SPLIT)),
            dma((GROUP, SPLIT)),
            dma((GROUP, SPLIT)),
            dma((2, SPLIT)),
            dma((2, SPLIT)),
            dma((2, 2, SPLIT)),
            pltpu.SemaphoreType.REGULAR,
        ],
        compiler_params=pltpu.CompilerParams(
            collective_id=0, has_side_effects=True, vmem_limit_bytes=64000000
        ),
    )(
        queries, key_rows, values, residual, w_out, w_gate, w_up, w_down, lambda_head,
        sub_gain.reshape(1, -1), norm_gain.reshape(1, -1), conv_gate, conv_up,
    )


def solution(mesh):
    placed = (
        P("sp", None),
        P("sp", "tp", None, None),
        P("sp", "tp", None, None),
        P("sp", "tp", None),
        P("tp"),
        P(),
        P("tp", None),
        P(),
        P("sp", "tp"),
        P("sp", "tp"),
        P(None, "tp"),
        P(None, "tp"),
        P("tp", None),
    )
    return jax.shard_map(
        functools.partial(local, mesh.shape["sp"], mesh.shape["tp"]),
        mesh=mesh, in_specs=placed, out_specs=P(("sp", "tp"), None), check_vma=False,
    )
```

```python
import contextlib
import functools
import math

import jax
import jax.numpy as jnp
from jax import lax
from jax.experimental import pallas as pl
from jax.experimental.pallas import tpu as pltpu
from jax.sharding import PartitionSpec as P

MESH = pl.DeviceIdType.MESH
epsilon = 1e-06
lambda_init = 0.8 - 0.6 * math.exp(-0.3)
bf16 = jnp.bfloat16
f32 = jnp.float32
HALO = 16
GROUP = 4
HUBS = (1, 2)
LANES = 128
SPLIT = 2
STAGED = {3: ((0, 0), (1, 0), (0, 1))}


def scope(name):
    return contextlib.nullcontext()


def parts_of(units):
    chunks = units // LANES
    first = (chunks + 1) // 2
    return ((0, first * LANES), (first * LANES, (chunks - first) * LANES))


def kernel(
    S, T, heads, dh, dv,
    q_hbm, k_hbm, v_hbm, res_hbm, wout_hbm, wg_hbm, wu_hbm, wd_hbm,
    lam_ref, sub_ref, norm_ref, cg_ref, cu_ref,
    out_ref,
    q_raw, k_raw, v_raw, q_out, kv_out, q, kv, res, wout, wg, wu, wd, stage,
    m_s, l_s, acc_s, n_own, n_in, part, part_in, mid, hn,
    g_s, u_s, halo_out, halo_in, hid, low, low_in, half, half_in, done, ret, home_out, home_in,
    local_sem, own_sem, pair_sem, kv_send, kv_recv,
    w_send, w_recv, cross_send, lend_send, stage_recv, stage_send, relay_send,
    tp_send, tp_recv, hn_send, hn_recv, ag_send, ag_recv,
    halo_send, halo_recv, core_send, core_recv, far_send, far_recv, ret_send, ret_recv, home_send, home_recv, go_sem,
):
    Z = S // 2
    sp = lax.axis_index("sp")
    tp = lax.axis_index("tp")
    z = lax.div(sp, 2)
    y = lax.rem(sp, 2)
    zi = lax.rem(z, GROUP)
    base = z - zi
    rows = q.shape[1]
    feat, units = wg_hbm.shape
    hh = heads // 2
    kw = 2 * hh * dh
    D = wout.shape[1]
    own = rows // T
    cap = wg.shape[1]
    pieces = parts_of(units)
    other = 1 - y
    mate = z * 2 + other
    has_up = z < Z - 1
    hub = (zi == HUBS[0]) | (zi == HUBS[1])
    core_mate = tp + 1 - 2 * lax.rem(tp, 2)
    far_mate = lax.rem(tp + 2, T)
    diagonal = T - 1 - tp

    def one(flag):
        return flag.astype(jnp.int32)

    def peer(d):
        return lax.rem(tp + d, T)

    def remote(src, dst, send, recv, device):
        return pltpu.make_async_remote_copy(
            src_ref=src, dst_ref=dst, send_sem=send, recv_sem=recv, device_id=device, device_id_type=MESH
        )

    def cols(k):
        return pl.ds(pieces[k][0], pieces[k][1])

    def block(b, k):
        return (pl.ds(pl.multiple_of(b * feat, feat), feat), pl.ds(0, pieces[k][1]))

    sources, stores = (wg_hbm, wu_hbm), (wg, wu)
    targets = [(g * GROUP + HUBS[k], k) for g in range(Z // GROUP) for k in range(2)]

    def direct(i, w):
        h, k = targets[i]
        return remote(
            sources[w].at[:, cols(k)], stores[w].at[block(sp, k)],
            w_send.at[w, i], w_recv.at[w, sp], (h * 2 + y, tp),
        )

    def cross(k, w):
        return remote(
            sources[w].at[:, cols(k)], stores[w].at[block(sp, k)],
            cross_send.at[w], w_recv.at[w, sp], (mate, tp),
        )

    def lend(k, w):
        return remote(
            sources[w].at[:, cols(k)], stage.at[k, w, :, pl.ds(0, pieces[k][1])],
            lend_send.at[k, w], stage_recv.at[k, w], (mate, tp),
        )

    def pass_on(k, w):
        h = base + HUBS[k]
        return remote(
            stage.at[k, w, :, pl.ds(0, pieces[k][1])], stores[w].at[block(mate, k)],
            stage_send.at[k, w], w_recv.at[w, mate], (h * 2 + y, tp),
        )

    def staged(zz, k, w):
        hit = zz < 0
        for zo, which in STAGED.items():
            if (k, w) in which:
                hit = hit | (zz == base + zo)
        return hit

    def each_staged(fn):
        for zo, which in STAGED.items():
            for k, w in which:
                pl.when(zi == zo)(functools.partial(fn, k, w))

    def relay(zz, k, w):
        b = zz * 2 + y
        return remote(
            stores[w].at[block(b, k)], stores[w].at[block(b, k)],
            relay_send.at[w, zz], w_recv.at[w, b], (mate, tp),
        )

    def own_piece(k, w):
        return pltpu.make_async_copy(sources[w].at[:, cols(k)], stores[w].at[block(sp, k)], own_sem.at[w])

    def down_piece(k):
        return pltpu.make_async_copy(
            wd_hbm.at[cols(k), :], wd.at[pl.ds(0, pieces[k][1]), :], own_sem.at[2]
        )

    def as_hub(fn):
        for k in range(2):
            pl.when(zi == HUBS[k])(functools.partial(fn, k))

    loads = [
        pltpu.make_async_copy(k_hbm, k_raw, local_sem.at[0]),
        pltpu.make_async_copy(v_hbm, v_raw, local_sem.at[4]),
        pltpu.make_async_copy(q_hbm, q_raw, local_sem.at[1]),
        pltpu.make_async_copy(wout_hbm, wout, local_sem.at[2]),
        pltpu.make_async_copy(res_hbm.at[pl.ds(pl.multiple_of(tp * own, own), own), :], res, local_sem.at[3]),
    ]
    for c in loads:
        c.start()

    def load_pieces(k):
        own_piece(k, 0).start()
        own_piece(k, 1).start()
        down_piece(k).start()

    as_hub(load_pieces)

    barrier = pltpu.get_barrier_semaphore()
    next_group, prev_group = (y == 1) & (z + GROUP < Z), (y == 0) & (z >= GROUP)

    def greet(device):
        pl.semaphore_signal(barrier, inc=1, device_id=device, device_id_type=MESH)

    with scope("barrier"):
        for zz in range(Z):
            pl.when(z != zz)(functools.partial(greet, (zz * 2 + y, tp)))
        greet((mate, tp))
        for d in range(1, T):
            greet((sp, peer(d)))
        pl.when(next_group)(lambda: greet((sp + 2 * GROUP - 1, tp)))
        pl.when(prev_group)(lambda: greet((sp - 2 * GROUP + 1, tp)))
        with scope("relayout"):
            for c in loads[:3]:
                c.wait()
            for yy in range(2):
                @pl.when(y == yy)
                def _():
                    for mine, q_to, kv_to in ((True, q.at[y], kv.at[sp]), (False, q_out, kv_out)):
                        for h in range(hh):
                            head = (yy if mine else 1 - yy) * hh + h
                            for c in range(2):
                                i = 2 * h + c
                                q_to[:, i * dh : (i + 1) * dh] = q_raw[:, head, c, :]
                                kv_to[:, i * dh : (i + 1) * dh] = k_raw[:, head, c, :]
                            kv_to[:, kw + h * dv : kw + (h + 1) * dv] = v_raw[:, head, :]
        pl.semaphore_wait(barrier, Z + T - 1 + one(next_group) + one(prev_group))

    def climb(blk):
        return remote(kv.at[blk], kv.at[blk], kv_send.at[blk], kv_recv.at[blk], (sp + 2, tp))

    def send_up(blk):
        pl.when(has_up)(lambda: climb(blk).start())

    def pair(src, dst, k):
        return remote(src, dst, pair_sem.at[0, k], pair_sem.at[1, k], (mate, tp))

    kv_swap = pair(kv_out, kv.at[sp], 0)
    q_swap = pair(q_out, q.at[y], 1)
    kv_got = pair(kv_out, kv.at[mate], 0)
    q_got = pair(q_out, q.at[other], 1)
    kv_swap.start()
    q_swap.start()
    send_up(sp)

    def direct_send(i):
        direct(i, 0).start()
        direct(i, 1).start()

    def second(h):
        return (zi == 3) & (h == z - 2)

    for i in reversed(range(len(targets))):
        h = targets[i][0]
        pl.when((z > h) & jnp.logical_not(second(h)))(functools.partial(direct_send, i))

    def cross_start(k):
        cross(k, 0).start()
        if k == 1:
            cross(k, 1).start()

    as_hub(cross_start)
    each_staged(lambda k, w: lend(k, w).start())

    def forward(k, w):
        lend(k, w).wait_recv()
        pass_on(k, w).start()

    m_s[...] = jnp.full(m_s.shape, -1e30, f32)
    l_s[...] = jnp.zeros(l_s.shape, f32)
    acc_s[...] = jnp.zeros(acc_s.shape, f32)
    scale = 1.0 / math.sqrt(dh)

    def clear_tail(k):
        lo, wide = pieces[k][1], cap - pieces[k][1]
        if wide:
            wg[:, lo:] = jnp.zeros((D, wide), bf16)
            wu[:, lo:] = jnp.zeros((D, wide), bf16)
            wd[lo:, :] = jnp.zeros((wide, D), bf16)

    as_hub(clear_tail)

    def attend(yy, blk):
        row_at = (z * 2 + yy) * rows + lax.broadcasted_iota(jnp.int32, (rows, rows), 0)
        col_at = blk * rows + lax.broadcasted_iota(jnp.int32, (rows, rows), 1)
        keep = col_at <= row_at
        for h in range(hh):
            v = kv[blk, :, kw + h * dv : kw + (h + 1) * dv]
            for c in range(2):
                i = 2 * h + c
                k = kv[blk, :, i * dh : (i + 1) * dh]
                s = lax.dot_general(
                    q[yy, :, i * dh : (i + 1) * dh], k, (((1,), (1,)), ((), ())),
                    preferred_element_type=f32,
                ) * scale
                s = jnp.where(keep, s, -1e30)
                old = m_s[yy, i]
                new = jnp.maximum(old, jnp.max(s, axis=1, keepdims=True))
                e = jnp.where(keep, jnp.exp(s - new), 0.0)
                fade = jnp.exp(old - new)
                m_s[yy, i] = new
                l_s[yy, i] = l_s[yy, i] * fade + jnp.sum(e, axis=1, keepdims=True)
                acc_s[yy, i] = acc_s[yy, i] * fade + jnp.dot(
                    e.astype(bf16), v, preferred_element_type=f32
                )

    def late(h):
        return (zi == 0) & (h > z + 1)

    def relay_from(zz, w):
        def go(k):
            @pl.when((zz != z) & jnp.logical_not(staged(zz, k, w)))
            def _():
                with scope("rly"):
                    relay(zz, k, w).wait_recv()
                relay(zz, k, w).start()

        as_hub(go)

    with scope("kvgot"):
        kv_got.wait_recv()
        send_up(mate)
        q_got.wait_recv()

    @pl.loop(0, Z)
    def _(r):
        @pl.when(z >= r)
        def _():
            @pl.when(r > 0)
            def _():
                for blk in (sp - 2 * r, mate - 2 * r):
                    with scope("arrkv"):
                        climb(blk).wait_recv()
                    send_up(blk)

            @pl.loop(0, 4)
            def _(i):
                yy, c = lax.div(i, 2), lax.rem(i, 2)
                with scope("attend"):
                    pl.when((r > 0) | (yy >= c))(lambda: attend(yy, (z - r) * 2 + c))

            @pl.when((r == 1) & (zi == HUBS[1]))
            def _():
                relay_from(z + 1, 1)

            @pl.when((r == 2) & (zi == 3))
            def _():
                forward(0, 0)

            @pl.when((r == 3) & (zi == 3))
            def _():
                forward(1, 0)
                forward(0, 1)

            for i in range(len(targets)):
                pl.when((r == 1) & second(targets[i][0]))(functools.partial(direct_send, i))

    for i in range(len(targets)):
        h = targets[i][0]
        pl.when((z < h) & jnp.logical_not(late(h)))(functools.partial(direct_send, i))

    with scope("nnorm"):
        for yy in range(2):
            for h in range(hh):
                a0 = acc_s[yy, 2 * h] / l_s[yy, 2 * h]
                a1 = acc_s[yy, 2 * h + 1] / l_s[yy, 2 * h + 1]
                a = a0 - lam_ref[y * hh + h] * a1
                ms = jnp.mean(a * a, axis=1, keepdims=True)
                n = a * lax.rsqrt(ms + epsilon) * sub_ref[...] * (1.0 - lambda_init)
                n_own[yy, :, h * dv : (h + 1) * dv] = n.astype(bf16)
    n_swap = pair(n_own.at[other], n_in, 2)
    n_swap.start()
    with scope("relay1"):
        @pl.when(zi == HUBS[0])
        def _():
            relay_from(z + 1, 0)
            cross(0, 1).start()

    with scope("nswapw"):
        loads[3].wait()
        n_swap.wait_recv()
    width = min(512, D)
    hw = hh * dv
    with scope("outproj"):
        for c in range(0, D, width):
            at = slice(c, c + width)
            part[:, :, at] = (
                (
                    jnp.dot(n_own[y], wout[pl.ds(y * hw, hw), at], preferred_element_type=f32)
                    + jnp.dot(n_in[...], wout[pl.ds(other * hw, hw), at], preferred_element_type=f32)
                )
                .astype(bf16)
                .reshape(T, own, width)
            )

    def swap(d):
        return remote(part.at[peer(d)], part_in.at[d], tp_send.at[d], tp_recv.at[d], (sp, peer(d)))

    firsts = [swap(d) for d in range(1, T)]
    for c in firsts:
        c.start()
    twin = jnp.where(zi == HUBS[0], z + 1, z - 1)
    with scope("relayt"):
        pl.when(zi == HUBS[1])(lambda: relay_from(twin, 0))
    with scope("rs1"):
        loads[4].wait()
        total = res[...].astype(f32) + part[tp].astype(f32)
        for d in range(1, T):
            firsts[d - 1].wait_recv()
            total = total + part_in[d].astype(f32)
        mid[...] = total
        ms = jnp.mean(total * total, axis=1, keepdims=True)

    def slot(p, t):
        return hn.at[p, pl.ds(pl.multiple_of(t * own, own), own)]

    hn[zi, pl.ds(pl.multiple_of(tp * own, own), own), :] = (
        total * lax.rsqrt(ms + epsilon) * norm_ref[...]
    ).astype(bf16)

    def deliver(k):
        return remote(
            slot(zi, tp), slot(zi, tp), hn_send.at[k], hn_recv.at[zi], ((base + HUBS[k]) * 2 + y, tp)
        )

    pl.when(zi != HUBS[0])(lambda: deliver(0).start())
    pl.when((zi == 0) | (zi == 3))(lambda: deliver(1).start())

    @pl.when(zi == 0)
    def _():
        pl.semaphore_wait(go_sem, 1)
        for i in range(len(targets)):
            pl.when(late(targets[i][0]))(functools.partial(direct_send, i))


    def spread(p, hop):
        src = (tp, tp, far_mate)[hop]
        to = (far_mate, core_mate, core_mate)[hop]
        return remote(slot(p, src), slot(p, src), ag_send.at[p, hop], ag_recv.at[p, hop], (sp, to))

    def gather1(p):
        @pl.when(p != zi)
        def _():
            remote(slot(p, tp), slot(p, tp), hn_send.at[0], hn_recv.at[p], (sp, tp)).wait_recv()

        spread(p, 0).start()
        spread(p, 1).start()

    def gather2(p):
        spread(p, 0).wait_recv()
        spread(p, 2).start()

    @pl.when(hub)
    def _():
        with scope("g1"):
            gather1(zi)

    with scope("relay2"):
        @pl.when(hub)
        def _():
            gather1(0)
            relay_from(twin, 1)
            for w in range(2):
                @pl.loop(0, Z)
                def _(i):
                    done_before = (Z - 1 - i == twin) | ((zi == HUBS[1]) & (Z - 1 - i == z + 1))
                    pl.when(jnp.logical_not(done_before))(lambda: relay_from(Z - 1 - i, w))

    def halo_copy(p):
        last = (y == 1) & (p == GROUP - 1)
        to = jnp.where(last, sp + 2 * GROUP - 1, mate)
        nxt = jnp.where(last, 0, p + y)
        return remote(
            halo_out.at[p], halo_in.at[nxt], halo_send.at[p], halo_recv.at[nxt], (to, tp)
        )

    def halo_sends(p):
        return (y == 0) | (p < GROUP - 1) | (z + GROUP < Z)

    side = D // SPLIT

    def span(h):
        return pl.ds(h * side, side)

    def core_copy(p, i, h):
        return remote(
            low.at[p, (core_mate, diagonal)[i], :, span(h)], low_in.at[p, i, :, span(h)],
            core_send.at[p, i, h], core_recv.at[p, i, h], (sp, core_mate),
        )

    def far_copy(p, h):
        return remote(
            half.at[p, :, span(h)], half_in.at[p, :, span(h)], far_send.at[p, h], far_recv.at[p, h],
            (sp, far_mate),
        )

    def give_back(p, k, h):
        return remote(
            done.at[p, :, span(h)], ret.at[k, :, span(h)], ret_send.at[p, h], ret_recv.at[k, h],
            ((base + p) * 2 + y, tp),
        )

    def reduce1(p, h):
        core_copy(p, 1, h).wait_recv()
        at = slice(h * side, (h + 1) * side)
        half[p, :, at] = (low[p, far_mate, :, at].astype(f32) + low_in[p, 1, :, at].astype(f32)).astype(bf16)
        far_copy(p, h).start()

    def home_copy(k, i, h):
        return remote(
            home_out.at[i, :, span(h)], home_in.at[k, i, :, span(h)],
            home_send.at[i, h], home_recv.at[k, i, h], (base * 2 + y, tp),
        )

    def send_home(h):
        at = slice(h * side, (h + 1) * side)
        for i, t in ((1, far_mate), (0, tp)):
            core_copy(0, i, h).wait_recv()
            home_out[i, :, at] = (low[0, t, :, at].astype(f32) + low_in[0, i, :, at].astype(f32)).astype(bf16)
            as_hub(lambda k: home_copy(k, i, h).start())

    def lift(h):
        return remote(
            done.at[GROUP - 1, :, span(h)], home_in.at[0, 0, :, span(h)],
            ret_send.at[GROUP - 1, h], home_recv.at[0, 0, h], ((base + HUBS[1]) * 2 + y, tp),
        )

    def reduce2(p, h):
        core_copy(p, 0, h).wait_recv()
        far_copy(p, h).wait_recv()
        at = slice(h * side, (h + 1) * side)
        t = low[p, tp, :, at].astype(f32) + low_in[p, 0, :, at].astype(f32) + half_in[p, :, at].astype(f32)

        def hand(k):
            if p == GROUP - 1 and k == 0:
                done[p, :, at] = t.astype(bf16)
                lift(h).start()
                return
            if p == GROUP - 1:
                lift(h).wait_recv()
                done[p, :, at] = (t + home_in[0, 0, :, at].astype(f32)).astype(bf16)
                give_back(p, k, h).start()
                return

            @pl.when(p == zi)
            def _():
                ret[k, :, at] = t.astype(bf16)

            @pl.when(p != zi)
            def _():
                done[p, :, at] = t.astype(bf16)
                give_back(p, k, h).start()

        as_hub(hand)

    def feed(p):
        wide = 256
        for c in range(0, cap, wide):
            at = slice(c, c + wide)
            g_s[HALO:, at] = jnp.dot(hn[p], wg[:, at], preferred_element_type=f32).astype(bf16).astype(f32)
            u_s[HALO:, at] = jnp.dot(hn[p], wu[:, at], preferred_element_type=f32).astype(bf16).astype(f32)
        halo_out[p, 0] = g_s[rows:, :].astype(bf16)
        halo_out[p, 1] = u_s[rows:, :].astype(bf16)
        pl.when(halo_sends(p))(lambda: halo_copy(p).start())

        lo = jnp.where(zi == HUBS[0], pieces[0][0], pieces[1][0])

        def conv(start, count):
            for c in range(0, cap, LANES):
                at = slice(c, c + LANES)
                tap = pl.ds(pl.multiple_of(jnp.minimum(lo + c, units - LANES), LANES), LANES)

                def mix(x, taps):
                    at0 = HALO + start
                    out = taps[0:1, tap] * x[at0 - 2 : at0 - 2 + count, at]
                    out = out + taps[1:2, tap] * x[at0 - 1 : at0 - 1 + count, at]
                    return out + taps[2:3, tap] * x[at0 : at0 + count, at]

                gm, um = mix(g_s, cg_ref), mix(u_s, cu_ref)
                hid[start : start + count, at] = (gm / (1.0 + jnp.exp(-gm)) * um).astype(bf16)

        @pl.when(p > 0)
        def _():
            @pl.when(p == 1)
            def _():
                for h in range(SPLIT):
                    send_home(h)

            @pl.when(p == 2)
            def _():
                for h in range(SPLIT):
                    reduce1(1, h)

        conv(HALO, rows - HALO)
        pl.when(p == GROUP - 2)(lambda: gather2(GROUP - 1))
        first = (y == 0) & (p == 0) & (base == 0)

        @pl.when(first)
        def _():
            g_s[:HALO, :] = jnp.zeros((HALO, cap), f32)
            u_s[:HALO, :] = jnp.zeros((HALO, cap), f32)

        @pl.when(jnp.logical_not(first))
        def _():
            with scope("halo"):
                remote(halo_out.at[p], halo_in.at[p], halo_send.at[p], halo_recv.at[p], (mate, tp)).wait_recv()
            g_s[:HALO, :] = halo_in[p, 0].astype(f32)
            u_s[:HALO, :] = halo_in[p, 1].astype(f32)

        conv(0, HALO)
        for c in range(0, D, width):
            at = slice(c, c + width)
            low[p, :, :, at] = (
                jnp.dot(hid[...], wd[:, at], preferred_element_type=f32).astype(bf16).reshape(T, own, width)
            )
            if (c + width) % side == 0:
                core_copy(p, 1, c // side).start()
                core_copy(p, 0, c // side).start()

    def wait_pieces(k):
        for w in range(2):
            own_piece(k, w).wait()

            def arrived(b):
              with scope("arrw"):
                remote(
                    stores[w].at[block(b, k)], stores[w].at[block(b, k)],
                    cross_send.at[w], w_recv.at[w, b], (mate, tp),
                ).wait_recv()

            @pl.loop(0, Z)
            def _(zz):
                pl.when(staged(zz, k, w))(lambda: arrived(zz * 2 + y))
                arrived(zz * 2 + other)

        down_piece(k).wait()

    with scope("go"):
        @pl.when(zi == HUBS[0])
        def _():
            for i in range(len(targets)):
                @pl.when(targets[i][0] == z + 1)
                def _():
                    with scope("gog"):
                        direct(i, 0).wait_send()
                    with scope("gou"):
                        direct(i, 1).wait_send()

            pl.semaphore_signal(go_sem, inc=1, device_id=(sp - 2, tp), device_id_type=MESH)
            deliver(1).start()

    @pl.when(hub)
    def _():
        with scope("ga"):
            gather2(zi)
            gather2(0)
            pl.when(zi == HUBS[0])(lambda: gather1(HUBS[1]))
            pl.when(zi == HUBS[1])(lambda: gather1(HUBS[0]))

        with scope("wwait"):
            as_hub(wait_pieces)

        @pl.loop(0, GROUP)
        def _(p):
            other_hub = jnp.where(zi == HUBS[0], HUBS[1], HUBS[0])
            with scope("gat"):
                pl.when(p == jnp.where(zi == HUBS[0], 1, 0))(lambda: gather1(GROUP - 1))
                pl.when(p == other_hub)(lambda: gather2(other_hub))
                pl.when(p == GROUP - 1)(lambda: reduce1(GROUP - 2, 0))

            with scope("agw"):
                spread(p, 1).wait_recv()
                spread(p, 2).wait_recv()
            with scope("feed"):
                feed(p)

        with scope("redlast"):
            for p, h in ((3, 0), (3, 1), (2, 1)):
                with scope("r1"):
                    reduce1(p, h)
            for p, h in ((1, 0), (1, 1), (2, 0), (3, 0), (3, 1), (2, 1)):
                with scope(f"r2{p}{h}"):
                    reduce2(p, h)

    with scope("final"):
        @pl.when(zi == 0)
        def _():
            for h in range(SPLIT):
                at = slice(h * side, (h + 1) * side)
                for k in range(2):
                    home_copy(k, 1, h).wait_recv()
                half[0, :, at] = (home_in[0, 1, :, at].astype(f32) + home_in[1, 1, :, at].astype(f32)).astype(bf16)
                far_copy(0, h).start()
            for h in range(SPLIT):
                at = slice(h * side, (h + 1) * side)
                for k in range(2):
                    home_copy(k, 0, h).wait_recv()
                total = mid[:, at] + home_in[0, 0, :, at].astype(f32) + home_in[1, 0, :, at].astype(f32)
                far_copy(0, h).wait_recv()
                out_ref[:, at] = (total + half_in[0, :, at].astype(f32)).astype(bf16)

        @pl.when(zi == GROUP - 1)
        def _():
            for h in range(SPLIT):
                at = slice(h * side, (h + 1) * side)
                remote(
                    done.at[0, :, span(h)], ret.at[1, :, span(h)], ret_send.at[0, h], ret_recv.at[1, h], (sp, tp)
                ).wait_recv()
                out_ref[:, at] = (mid[:, at] + ret[1, :, at].astype(f32)).astype(bf16)

        @pl.when(hub)
        def _():
            for h in range(SPLIT):
                at = slice(h * side, (h + 1) * side)
                total = mid[:, at]
                for k in range(2):
                    got = remote(
                        done.at[0, :, span(h)], ret.at[k, :, span(h)], ret_send.at[0, h], ret_recv.at[k, h], (sp, tp)
                    )
                    pl.when(zi != HUBS[k])(got.wait_recv)
                    total = total + ret[k, :, at].astype(f32)
                out_ref[:, at] = total.astype(bf16)

    with scope("drain"):
        @pl.loop(0, Z)
        def _(zz):
            @pl.when(has_up & (zz <= z))
            def _():
                climb(2 * zz).wait_send()
                climb(2 * zz + 1).wait_send()

            def go(k):
                for w in range(2):
                    pl.when((zz != z) & jnp.logical_not(staged(zz, k, w)))(relay(zz, k, w).wait_send)

            as_hub(go)

        for i in range(len(targets)):
            @pl.when((z != targets[i][0]) & ((zi != HUBS[0]) | (targets[i][0] != z + 1)))
            def _():
                direct(i, 0).wait_send()
                direct(i, 1).wait_send()

        def cross_end(k):
            cross(k, 0).wait_send()
            cross(k, 1).wait_send()

        as_hub(cross_end)

        def lend_end(k, w):
            lend(k, w).wait_send()
            pass_on(k, w).wait_send()

        each_staged(lend_end)
        for c in firsts + [kv_swap, q_swap, n_swap]:
            c.wait_send()
        for k in range(2):
            pl.when(zi != HUBS[k])(lambda: deliver(k).wait_send())

        @pl.when(zi == 0)
        def _():
            for h in range(SPLIT):
                far_copy(0, h).wait_send()

        @pl.when(hub)
        def _():
            for h in range(SPLIT):
                for i in range(2):
                    home_copy(0, i, h).wait_send()

            @pl.loop(0, GROUP)
            def _(p):
                for hop in range(3):
                    spread(p, hop).wait_send()
                pl.when(halo_sends(p))(lambda: halo_copy(p).wait_send())
                for h in range(SPLIT):
                    core_copy(p, 0, h).wait_send()
                    core_copy(p, 1, h).wait_send()
                    pl.when(p > 0)(far_copy(p, h).wait_send)
                    pl.when((p > 0) & (p != zi))(give_back(p, 0, h).wait_send)


def local(
    S, T,
    residual, queries, key_rows, values, lambda_head, sub_gain, w_out, norm_gain,
    w_gate, w_up, conv_gate, conv_up, w_down,
):
    rows, heads, maps, dh = queries.shape
    dv = values.shape[2]
    feat, units = w_gate.shape
    D = w_out.shape[1]
    own = rows // T
    cap = max(p[1] for p in parts_of(units))
    hh = heads // 2
    qw = hh * maps * dh
    kvw = qw + hh * dv
    Z = S // 2
    hbm = pl.BlockSpec(memory_space=pl.ANY)
    vmem = pl.BlockSpec(memory_space=pltpu.VMEM)
    smem = pl.BlockSpec(memory_space=pltpu.SMEM)
    V = pltpu.VMEM
    dma = pltpu.SemaphoreType.DMA
    return pl.pallas_call(
        functools.partial(kernel, S, T, heads, dh, dv),
        out_shape=jax.ShapeDtypeStruct((own, D), bf16),
        in_specs=[hbm] * 8 + [smem] + [vmem] * 4,
        out_specs=vmem,
        scratch_shapes=[
            V(queries.shape, bf16),
            V(key_rows.shape, bf16),
            V(values.shape, bf16),
            V((rows, qw), bf16),
            V((rows, kvw), bf16),
            V((2, rows, qw), bf16),
            V((S, rows, kvw), bf16),
            V((own, D), bf16),
            V(w_out.shape, bf16),
            V((D, cap), bf16),
            V((D, cap), bf16),
            V((cap, D), bf16),
            V((2, 2, feat, cap), bf16),
            V((2, 2 * hh, rows, 1), f32),
            V((2, 2 * hh, rows, 1), f32),
            V((2, 2 * hh, rows, dv), f32),
            V((2, rows, hh * dv), bf16),
            V((rows, hh * dv), bf16),
            V((T, own, D), bf16),
            V((T, own, D), bf16),
            V((own, D), f32),
            V((GROUP, rows, D), bf16),
            V((rows + HALO, cap), f32),
            V((rows + HALO, cap), f32),
            V((GROUP, 2, HALO, cap), bf16),
            V((GROUP, 2, HALO, cap), bf16),
            V((rows, cap), bf16),
            V((GROUP, T, own, D), bf16),
            V((GROUP, 2, own, D), bf16),
            V((GROUP, own, D), bf16),
            V((GROUP, own, D), bf16),
            V((GROUP, own, D), bf16),
            V((2, own, D), bf16),
            V((2, own, D), bf16),
            V((2, 2, own, D), bf16),
            dma((5,)),
            dma((3,)),
            dma((2, 3)),
            dma((S,)),
            dma((S,)),
            dma((2, Z // 2)),
            dma((2, S)),
            dma((2,)),
            dma((2, 2)),
            dma((2, 2)),
            dma((2, 2)),
            dma((2, Z)),
            dma((T,)),
            dma((T,)),
            dma((2,)),
            dma((GROUP,)),
            dma((GROUP, 3)),
            dma((GROUP, 3)),
            dma((GROUP,)),
            dma((GROUP,)),
            dma((GROUP, 2, SPLIT)),
            dma((GROUP, 2, SPLIT)),
            dma((GROUP, SPLIT)),
            dma((GROUP, SPLIT)),
            dma((GROUP, SPLIT)),
            dma((2, SPLIT)),
            dma((2, SPLIT)),
            dma((2, 2, SPLIT)),
            pltpu.SemaphoreType.REGULAR,
        ],
        compiler_params=pltpu.CompilerParams(
            collective_id=0, has_side_effects=True, vmem_limit_bytes=64000000
        ),
    )(
        queries, key_rows, values, residual, w_out, w_gate, w_up, w_down, lambda_head,
        sub_gain.reshape(1, -1), norm_gain.reshape(1, -1), conv_gate, conv_up,
    )


def solution(mesh):
    placed = (
        P("sp", None),
        P("sp", "tp", None, None),
        P("sp", "tp", None, None),
        P("sp", "tp", None),
        P("tp"),
        P(),
        P("tp", None),
        P(),
        P("sp", "tp"),
        P("sp", "tp"),
        P(None, "tp"),
        P(None, "tp"),
        P("tp", None),
    )
    return jax.shard_map(
        functools.partial(local, mesh.shape["sp"], mesh.shape["tp"]),
        mesh=mesh, in_specs=placed, out_specs=P(("sp", "tp"), None), check_vma=False,
    )
```

```python
import contextlib
import functools
import math

import jax
import jax.numpy as jnp
from jax import lax
from jax.experimental import pallas as pl
from jax.experimental.pallas import tpu as pltpu
from jax.sharding import PartitionSpec as P

MESH = pl.DeviceIdType.MESH
epsilon = 1e-06
lambda_init = 0.8 - 0.6 * math.exp(-0.3)
bf16 = jnp.bfloat16
f32 = jnp.float32
HALO = 16
GROUP = 4
HUBS = (1, 2)
LANES = 128
SPLIT = 2
STAGED = {3: ((0, 0), (1, 0), (0, 1))}


def scope(name):
    return contextlib.nullcontext()


def parts_of(units):
    chunks = units // LANES
    first = (chunks + 1) // 2
    return ((0, first * LANES), (first * LANES, (chunks - first) * LANES))


def kernel(
    S, T, heads, dh, dv,
    q_hbm, k_hbm, v_hbm, res_hbm, wout_hbm, wg_hbm, wu_hbm, wd_hbm,
    lam_ref, sub_ref, norm_ref, cg_ref, cu_ref,
    out_ref,
    q_raw, k_raw, v_raw, q_out, kv_out, q, kv, res, wout, wg, wu, wd, stage,
    m_s, l_s, acc_s, n_own, n_in, part, part_in, mid, hn,
    g_s, u_s, halo_out, halo_in, hid, low, low_in, half, half_in, done, ret, home_out, home_in,
    local_sem, own_sem, pair_sem, kv_send, kv_recv,
    w_send, w_recv, cross_send, lend_send, stage_recv, stage_send, relay_send,
    tp_send, tp_recv, hn_send, hn_recv, ag_send, ag_recv,
    halo_send, halo_recv, core_send, core_recv, far_send, far_recv, ret_send, ret_recv, home_send, home_recv, go_sem, mate_sem,
):
    Z = S // 2
    sp = lax.axis_index("sp")
    tp = lax.axis_index("tp")
    z = lax.div(sp, 2)
    y = lax.rem(sp, 2)
    zi = lax.rem(z, GROUP)
    base = z - zi
    rows = q.shape[1]
    feat, units = wg_hbm.shape
    hh = heads // 2
    kw = 2 * hh * dh
    D = wout.shape[1]
    own = rows // T
    cap = wg.shape[1]
    pieces = parts_of(units)
    other = 1 - y
    mate = z * 2 + other
    has_up = z < Z - 1
    hub = (zi == HUBS[0]) | (zi == HUBS[1])
    core_mate = tp + 1 - 2 * lax.rem(tp, 2)
    far_mate = lax.rem(tp + 2, T)
    diagonal = T - 1 - tp

    def one(flag):
        return flag.astype(jnp.int32)

    def peer(d):
        return lax.rem(tp + d, T)

    def remote(src, dst, send, recv, device):
        return pltpu.make_async_remote_copy(
            src_ref=src, dst_ref=dst, send_sem=send, recv_sem=recv, device_id=device, device_id_type=MESH
        )

    def cols(k):
        return pl.ds(pieces[k][0], pieces[k][1])

    cut = feat // 2

    def part_rows(w):
        return pl.ds((w % 2) * cut, cut)

    def block(b, k, w):
        return (pl.ds(pl.multiple_of(b * feat + (w % 2) * cut, cut), cut), pl.ds(0, pieces[k][1]))

    sources, stores = (wg_hbm, wu_hbm), (wg, wu)
    targets = [(g * GROUP + HUBS[k], k) for g in range(Z // GROUP) for k in range(2)]

    def direct(i, w):
        h, k = targets[i]
        return remote(
            sources[w // 2].at[part_rows(w), cols(k)], stores[w // 2].at[block(sp, k, w)],
            w_send.at[w, i], w_recv.at[w, sp], (h * 2 + y, tp),
        )

    def cross(k, w):
        return remote(
            sources[w // 2].at[part_rows(w), cols(k)], stores[w // 2].at[block(sp, k, w)],
            cross_send.at[w], w_recv.at[w, sp], (mate, tp),
        )

    def lend(k, w):
        return remote(
            sources[w // 2].at[part_rows(w), cols(k)], stage.at[k, w // 2, part_rows(w), pl.ds(0, pieces[k][1])],
            lend_send.at[k, w], stage_recv.at[k, w], (mate, tp),
        )

    def pass_on(k, w):
        h = base + HUBS[k]
        return remote(
            stage.at[k, w // 2, part_rows(w), pl.ds(0, pieces[k][1])], stores[w // 2].at[block(mate, k, w)],
            stage_send.at[k, w], w_recv.at[w, mate], (h * 2 + y, tp),
        )

    def staged(zz, k, w):
        hit = zz < 0
        for zo, which in STAGED.items():
            if (k, w // 2) in which:
                hit = hit | (zz == base + zo)
        return hit

    def each_staged(fn):
        for zo, which in STAGED.items():
            for k, w in which:
                pl.when(zi == zo)(functools.partial(fn, k, 2 * w))
                pl.when(zi == zo)(functools.partial(fn, k, 2 * w + 1))

    def relay(zz, k, w):
        b = zz * 2 + y
        return remote(
            stores[w // 2].at[block(b, k, w)], stores[w // 2].at[block(b, k, w)],
            relay_send.at[w, zz], w_recv.at[w, b], (mate, tp),
        )

    def own_piece(k, w):
        return pltpu.make_async_copy(sources[w].at[:, cols(k)], stores[w].at[pl.ds(pl.multiple_of(sp * feat, feat), feat), pl.ds(0, pieces[k][1])], own_sem.at[w])

    def down_piece(k):
        return pltpu.make_async_copy(
            wd_hbm.at[cols(k), :], wd.at[pl.ds(0, pieces[k][1]), :], own_sem.at[2]
        )

    def as_hub(fn):
        for k in range(2):
            pl.when(zi == HUBS[k])(functools.partial(fn, k))

    loads = [
        pltpu.make_async_copy(k_hbm, k_raw, local_sem.at[0]),
        pltpu.make_async_copy(v_hbm, v_raw, local_sem.at[4]),
        pltpu.make_async_copy(q_hbm, q_raw, local_sem.at[1]),
        pltpu.make_async_copy(wout_hbm, wout, local_sem.at[2]),
        pltpu.make_async_copy(res_hbm.at[pl.ds(pl.multiple_of(tp * own, own), own), :], res, local_sem.at[3]),
    ]
    for c in loads:
        c.start()

    def load_pieces(k):
        own_piece(k, 0).start()
        own_piece(k, 1).start()
        down_piece(k).start()

    as_hub(load_pieces)

    barrier = pltpu.get_barrier_semaphore()
    next_group, prev_group = (y == 1) & (z + GROUP < Z), (y == 0) & (z >= GROUP)

    def greet(device):
        pl.semaphore_signal(barrier, inc=1, device_id=device, device_id_type=MESH)

    with scope("barrier"):
        for zz in range(Z):
            pl.when(z != zz)(functools.partial(greet, (zz * 2 + y, tp)))
        greet((mate, tp))
        for d in range(1, T):
            greet((sp, peer(d)))
        pl.when(next_group)(lambda: greet((sp + 2 * GROUP - 1, tp)))
        pl.when(prev_group)(lambda: greet((sp - 2 * GROUP + 1, tp)))
        with scope("relayout"):
            for c in loads[:3]:
                c.wait()
            for yy in range(2):
                @pl.when(y == yy)
                def _():
                    for mine, q_to, kv_to in ((True, q.at[y], kv.at[sp]), (False, q_out, kv_out)):
                        for h in range(hh):
                            head = (yy if mine else 1 - yy) * hh + h
                            for c in range(2):
                                i = 2 * h + c
                                q_to[:, i * dh : (i + 1) * dh] = q_raw[:, head, c, :]
                                kv_to[:, i * dh : (i + 1) * dh] = k_raw[:, head, c, :]
                            kv_to[:, kw + h * dv : kw + (h + 1) * dv] = v_raw[:, head, :]
        pl.semaphore_wait(barrier, Z + T - 1 + one(next_group) + one(prev_group))

    def climb(blk):
        return remote(kv.at[blk], kv.at[blk], kv_send.at[blk], kv_recv.at[blk], (sp + 2, tp))

    def send_up(blk):
        pl.when(has_up)(lambda: climb(blk).start())

    def pair(src, dst, k):
        return remote(src, dst, pair_sem.at[0, k], pair_sem.at[1, k], (mate, tp))

    kv_swap = pair(kv_out, kv.at[sp], 0)
    q_swap = pair(q_out, q.at[y], 1)
    kv_got = pair(kv_out, kv.at[mate], 0)
    q_got = pair(q_out, q.at[other], 1)
    kv_swap.start()
    q_swap.start()
    send_up(sp)

    def direct_send(i):
        for w in range(4):
            direct(i, w).start()

    def second(h):
        return (zi == 3) & (h == z - 2)

    for i in reversed(range(len(targets))):
        h = targets[i][0]
        pl.when((z > h) & jnp.logical_not(second(h)))(functools.partial(direct_send, i))

    def cross_start(k):
        for w in range(4 if k == 1 else 2):
            cross(k, w).start()

    as_hub(cross_start)
    each_staged(lambda k, w: lend(k, w).start())

    def forward(k, w):
        for part in (2 * w, 2 * w + 1):
            lend(k, part).wait_recv()
            pass_on(k, part).start()

    m_s[...] = jnp.full(m_s.shape, -1e30, f32)
    l_s[...] = jnp.zeros(l_s.shape, f32)
    acc_s[...] = jnp.zeros(acc_s.shape, f32)
    scale = 1.0 / math.sqrt(dh)

    def clear_tail(k):
        lo, wide = pieces[k][1], cap - pieces[k][1]
        if wide:
            wg[:, lo:] = jnp.zeros((D, wide), bf16)
            wu[:, lo:] = jnp.zeros((D, wide), bf16)
            wd[lo:, :] = jnp.zeros((wide, D), bf16)

    as_hub(clear_tail)

    def attend(yy, blk):
        row_at = (z * 2 + yy) * rows + lax.broadcasted_iota(jnp.int32, (rows, rows), 0)
        col_at = blk * rows + lax.broadcasted_iota(jnp.int32, (rows, rows), 1)
        keep = col_at <= row_at
        for h in range(hh):
            v = kv[blk, :, kw + h * dv : kw + (h + 1) * dv]
            for c in range(2):
                i = 2 * h + c
                k = kv[blk, :, i * dh : (i + 1) * dh]
                s = lax.dot_general(
                    q[yy, :, i * dh : (i + 1) * dh], k, (((1,), (1,)), ((), ())),
                    preferred_element_type=f32,
                ) * scale
                s = jnp.where(keep, s, -1e30)
                old = m_s[yy, i]
                new = jnp.maximum(old, jnp.max(s, axis=1, keepdims=True))
                e = jnp.where(keep, jnp.exp(s - new), 0.0)
                fade = jnp.exp(old - new)
                m_s[yy, i] = new
                l_s[yy, i] = l_s[yy, i] * fade + jnp.sum(e, axis=1, keepdims=True)
                acc_s[yy, i] = acc_s[yy, i] * fade + jnp.dot(
                    e.astype(bf16), v, preferred_element_type=f32
                )

    def late(h):
        return (zi == 0) & (h > z + 1)

    def relay_from(zz, which):
        def go(k):
            @pl.when((zz != z) & jnp.logical_not(staged(zz, k, 2 * which)))
            def _():
                for w in (2 * which, 2 * which + 1):
                    with scope("rly"):
                        relay(zz, k, w).wait_recv()
                    relay(zz, k, w).start()

        as_hub(go)

    with scope("kvgot"):
        kv_got.wait_recv()
        send_up(mate)
        q_got.wait_recv()

    @pl.loop(0, Z)
    def _(r):
        @pl.when(z >= r)
        def _():
            @pl.when(r > 0)
            def _():
                for blk in (sp - 2 * r, mate - 2 * r):
                    with scope("arrkv"):
                        climb(blk).wait_recv()
                    send_up(blk)

            @pl.loop(0, 4)
            def _(i):
                yy, c = lax.div(i, 2), lax.rem(i, 2)
                with scope("attend"):
                    pl.when((r > 0) | (yy >= c))(lambda: attend(yy, (z - r) * 2 + c))

            @pl.when((r == 1) & (zi == HUBS[1]))
            def _():
                relay_from(z + 1, 1)

            @pl.when((r == 2) & (zi == 3))
            def _():
                forward(0, 0)

            @pl.when((r == 3) & (zi == 3))
            def _():
                forward(1, 0)
                forward(0, 1)

            for i in range(len(targets)):
                pl.when((r == 1) & second(targets[i][0]))(functools.partial(direct_send, i))

    for i in range(len(targets)):
        h = targets[i][0]
        pl.when((z < h) & jnp.logical_not(late(h)))(functools.partial(direct_send, i))

    with scope("nnorm"):
        for yy in range(2):
            for h in range(hh):
                a0 = acc_s[yy, 2 * h] / l_s[yy, 2 * h]
                a1 = acc_s[yy, 2 * h + 1] / l_s[yy, 2 * h + 1]
                a = a0 - lam_ref[y * hh + h] * a1
                ms = jnp.mean(a * a, axis=1, keepdims=True)
                n = a * lax.rsqrt(ms + epsilon) * sub_ref[...] * (1.0 - lambda_init)
                n_own[yy, :, h * dv : (h + 1) * dv] = n.astype(bf16)
    n_swap = pair(n_own.at[other], n_in, 2)
    n_swap.start()
    with scope("relay1"):
        @pl.when(zi == HUBS[0])
        def _():
            relay_from(z + 1, 0)
            cross(0, 2).start()
            cross(0, 3).start()

    with scope("nswapw"):
        loads[3].wait()
        n_swap.wait_recv()
    width = min(512, D)
    hw = hh * dv
    with scope("outproj"):
        for c in range(0, D, width):
            at = slice(c, c + width)
            part[:, :, at] = (
                (
                    jnp.dot(n_own[y], wout[pl.ds(y * hw, hw), at], preferred_element_type=f32)
                    + jnp.dot(n_in[...], wout[pl.ds(other * hw, hw), at], preferred_element_type=f32)
                )
                .astype(bf16)
                .reshape(T, own, width)
            )

    def swap(d):
        return remote(part.at[peer(d)], part_in.at[d], tp_send.at[d], tp_recv.at[d], (sp, peer(d)))

    firsts = [swap(d) for d in range(1, T)]
    for c in firsts:
        c.start()
    twin = jnp.where(zi == HUBS[0], z + 1, z - 1)
    with scope("relayt"):
        pl.when(zi == HUBS[1])(lambda: relay_from(twin, 0))
    with scope("rs1"):
        loads[4].wait()
        total = res[...].astype(f32) + part[tp].astype(f32)
        for d in range(1, T):
            firsts[d - 1].wait_recv()
            total = total + part_in[d].astype(f32)
        mid[...] = total
        ms = jnp.mean(total * total, axis=1, keepdims=True)

    def slot(p, t):
        return hn.at[p, pl.ds(pl.multiple_of(t * own, own), own)]

    hn[zi, pl.ds(pl.multiple_of(tp * own, own), own), :] = (
        total * lax.rsqrt(ms + epsilon) * norm_ref[...]
    ).astype(bf16)

    def deliver(k):
        return remote(
            slot(zi, tp), slot(zi, tp), hn_send.at[k], hn_recv.at[zi], ((base + HUBS[k]) * 2 + y, tp)
        )

    pl.when(zi != HUBS[0])(lambda: deliver(0).start())
    pl.when((zi == 0) | (zi == 3))(lambda: deliver(1).start())

    @pl.when(zi == 0)
    def _():
        pl.semaphore_wait(go_sem, 1)
        for i in range(len(targets)):
            pl.when(late(targets[i][0]))(functools.partial(direct_send, i))


    def spread(p, hop):
        src = (tp, tp, far_mate)[hop]
        to = (far_mate, core_mate, core_mate)[hop]
        return remote(slot(p, src), slot(p, src), ag_send.at[p, hop], ag_recv.at[p, hop], (sp, to))

    def gather1(p):
        @pl.when(p != zi)
        def _():
            remote(slot(p, tp), slot(p, tp), hn_send.at[0], hn_recv.at[p], (sp, tp)).wait_recv()

        spread(p, 0).start()
        spread(p, 1).start()

    def gather2(p):
        spread(p, 0).wait_recv()
        spread(p, 2).start()

    @pl.when(hub)
    def _():
        with scope("g1"):
            gather1(zi)

    with scope("relay2"):
        @pl.when(hub)
        def _():
            gather1(0)
            relay_from(twin, 1)
            for w in range(2):
                @pl.loop(0, Z)
                def _(i):
                    done_before = (Z - 1 - i == twin) | ((zi == HUBS[1]) & (Z - 1 - i == z + 1))
                    pl.when(jnp.logical_not(done_before))(lambda: relay_from(Z - 1 - i, w))

    def halo_copy(p):
        last = (y == 1) & (p == GROUP - 1)
        to = jnp.where(last, sp + 2 * GROUP - 1, mate)
        nxt = jnp.where(last, 0, p + y)
        return remote(
            halo_out.at[p], halo_in.at[nxt], halo_send.at[p], halo_recv.at[nxt], (to, tp)
        )

    def halo_sends(p):
        return (y == 0) | (p < GROUP - 1) | (z + GROUP < Z)

    side = D // SPLIT

    def span(h):
        return pl.ds(h * side, side)

    def core_copy(p, i, h):
        return remote(
            low.at[p, (core_mate, diagonal)[i], :, span(h)], low_in.at[p, i, :, span(h)],
            core_send.at[p, i, h], core_recv.at[p, i, h], (sp, core_mate),
        )

    def far_copy(p, h):
        return remote(
            half.at[p, :, span(h)], half_in.at[p, :, span(h)], far_send.at[p, h], far_recv.at[p, h],
            (sp, far_mate),
        )

    def give_back(p, k, h):
        return remote(
            done.at[p, :, span(h)], ret.at[k, :, span(h)], ret_send.at[p, h], ret_recv.at[k, h],
            ((base + p) * 2 + y, tp),
        )

    def reduce1(p, h):
        core_copy(p, 1, h).wait_recv()
        at = slice(h * side, (h + 1) * side)
        half[p, :, at] = (low[p, far_mate, :, at].astype(f32) + low_in[p, 1, :, at].astype(f32)).astype(bf16)
        far_copy(p, h).start()

    def home_copy(k, i, h):
        return remote(
            home_out.at[i, :, span(h)], home_in.at[k, i, :, span(h)],
            home_send.at[i, h], home_recv.at[k, i, h], (base * 2 + y, tp),
        )

    def send_home(h):
        at = slice(h * side, (h + 1) * side)
        for i, t in ((1, far_mate), (0, tp)):
            core_copy(0, i, h).wait_recv()
            home_out[i, :, at] = (low[0, t, :, at].astype(f32) + low_in[0, i, :, at].astype(f32)).astype(bf16)
            as_hub(lambda k: home_copy(k, i, h).start())

    def lift(h):
        return remote(
            done.at[GROUP - 1, :, span(h)], home_in.at[0, 0, :, span(h)],
            ret_send.at[GROUP - 1, h], home_recv.at[0, 0, h], ((base + HUBS[1]) * 2 + y, tp),
        )

    def reduce2(p, h):
        core_copy(p, 0, h).wait_recv()
        far_copy(p, h).wait_recv()
        at = slice(h * side, (h + 1) * side)
        t = low[p, tp, :, at].astype(f32) + low_in[p, 0, :, at].astype(f32) + half_in[p, :, at].astype(f32)

        def hand(k):
            if p == GROUP - 1 and k == 0:
                done[p, :, at] = t.astype(bf16)
                lift(h).start()
                return
            if p == GROUP - 1:
                lift(h).wait_recv()
                done[p, :, at] = (t + home_in[0, 0, :, at].astype(f32)).astype(bf16)
                give_back(p, k, h).start()
                return

            @pl.when(p == zi)
            def _():
                ret[k, :, at] = t.astype(bf16)

            @pl.when(p != zi)
            def _():
                done[p, :, at] = t.astype(bf16)
                give_back(p, k, h).start()

        as_hub(hand)

    def feed(p):
        wide = 256
        for c in range(0, cap, wide):
            at = slice(c, c + wide)
            g_s[HALO:, at] = jnp.dot(hn[p], wg[:, at], preferred_element_type=f32).astype(bf16).astype(f32)
            u_s[HALO:, at] = jnp.dot(hn[p], wu[:, at], preferred_element_type=f32).astype(bf16).astype(f32)
        halo_out[p, 0] = g_s[rows:, :].astype(bf16)
        halo_out[p, 1] = u_s[rows:, :].astype(bf16)
        pl.when(halo_sends(p))(lambda: halo_copy(p).start())

        lo = jnp.where(zi == HUBS[0], pieces[0][0], pieces[1][0])

        def conv(start, count):
            for c in range(0, cap, LANES):
                at = slice(c, c + LANES)
                tap = pl.ds(pl.multiple_of(jnp.minimum(lo + c, units - LANES), LANES), LANES)

                def mix(x, taps):
                    at0 = HALO + start
                    out = taps[0:1, tap] * x[at0 - 2 : at0 - 2 + count, at]
                    out = out + taps[1:2, tap] * x[at0 - 1 : at0 - 1 + count, at]
                    return out + taps[2:3, tap] * x[at0 : at0 + count, at]

                gm, um = mix(g_s, cg_ref), mix(u_s, cu_ref)
                hid[start : start + count, at] = (gm / (1.0 + jnp.exp(-gm)) * um).astype(bf16)

        @pl.when(p > 0)
        def _():
            @pl.when(p == 1)
            def _():
                for h in range(SPLIT):
                    send_home(h)

            @pl.when(p == 2)
            def _():
                for h in range(SPLIT):
                    reduce1(1, h)

        conv(HALO, rows - HALO)
        pl.when(p == GROUP - 2)(lambda: gather2(GROUP - 1))
        first = (y == 0) & (p == 0) & (base == 0)

        @pl.when(first)
        def _():
            g_s[:HALO, :] = jnp.zeros((HALO, cap), f32)
            u_s[:HALO, :] = jnp.zeros((HALO, cap), f32)

        @pl.when(jnp.logical_not(first))
        def _():
            with scope("halo"):
                remote(halo_out.at[p], halo_in.at[p], halo_send.at[p], halo_recv.at[p], (mate, tp)).wait_recv()
            g_s[:HALO, :] = halo_in[p, 0].astype(f32)
            u_s[:HALO, :] = halo_in[p, 1].astype(f32)

        conv(0, HALO)
        for c in range(0, D, width):
            at = slice(c, c + width)
            low[p, :, :, at] = (
                jnp.dot(hid[...], wd[:, at], preferred_element_type=f32).astype(bf16).reshape(T, own, width)
            )
            if (c + width) % side == 0:
                core_copy(p, 1, c // side).start()
                core_copy(p, 0, c // side).start()

    def wait_pieces(k):
        own_piece(k, 0).wait()
        own_piece(k, 1).wait()
        for w in range(4):

            def arrived(b):
                remote(
                    stores[w // 2].at[block(b, k, w)], stores[w // 2].at[block(b, k, w)],
                    cross_send.at[w], w_recv.at[w, b], (mate, tp),
                ).wait_recv()

            @pl.loop(0, Z)
            def _(zz):
                pl.when(staged(zz, k, w))(lambda: arrived(zz * 2 + y))
                arrived(zz * 2 + other)

        down_piece(k).wait()

    with scope("go"):
        @pl.when(zi == HUBS[0])
        def _():
            for i in range(len(targets)):
                @pl.when(targets[i][0] == z + 1)
                def _():
                    for w in range(4):
                        direct(i, w).wait_send()

            pl.semaphore_signal(mate_sem, inc=1, device_id=(sp, core_mate), device_id_type=MESH)
            pl.semaphore_wait(mate_sem, 1)
            pl.semaphore_signal(go_sem, inc=1, device_id=(sp - 2, tp), device_id_type=MESH)
            deliver(1).start()

    @pl.when(hub)
    def _():
        with scope("ga"):
            gather2(zi)
            gather2(0)
            pl.when(zi == HUBS[0])(lambda: gather1(HUBS[1]))
            pl.when(zi == HUBS[1])(lambda: gather1(HUBS[0]))

        with scope("wwait"):
            as_hub(wait_pieces)

        @pl.loop(0, GROUP)
        def _(p):
            other_hub = jnp.where(zi == HUBS[0], HUBS[1], HUBS[0])
            with scope("gat"):
                pl.when(p == 1)(lambda: gather1(GROUP - 1))
                pl.when(p == other_hub)(lambda: gather2(other_hub))
                pl.when(p == GROUP - 1)(lambda: reduce1(GROUP - 2, 0))

            with scope("agw"):
                spread(p, 1).wait_recv()
                spread(p, 2).wait_recv()
            with scope("feed"):
                feed(p)

        with scope("redlast"):
            for p, h in ((3, 0), (3, 1), (2, 1)):
                with scope("r1"):
                    reduce1(p, h)
            for p, h in ((1, 0), (1, 1), (2, 0), (3, 0), (3, 1), (2, 1)):
                with scope(f"r2{p}{h}"):
                    reduce2(p, h)

    with scope("final"):
        @pl.when(zi == 0)
        def _():
            for h in range(SPLIT):
                at = slice(h * side, (h + 1) * side)
                for k in range(2):
                    home_copy(k, 1, h).wait_recv()
                half[0, :, at] = (home_in[0, 1, :, at].astype(f32) + home_in[1, 1, :, at].astype(f32)).astype(bf16)
                far_copy(0, h).start()
            for h in range(SPLIT):
                at = slice(h * side, (h + 1) * side)
                for k in range(2):
                    home_copy(k, 0, h).wait_recv()
                total = mid[:, at] + home_in[0, 0, :, at].astype(f32) + home_in[1, 0, :, at].astype(f32)
                far_copy(0, h).wait_recv()
                out_ref[:, at] = (total + half_in[0, :, at].astype(f32)).astype(bf16)

        @pl.when(zi == GROUP - 1)
        def _():
            for h in range(SPLIT):
                at = slice(h * side, (h + 1) * side)
                remote(
                    done.at[0, :, span(h)], ret.at[1, :, span(h)], ret_send.at[0, h], ret_recv.at[1, h], (sp, tp)
                ).wait_recv()
                out_ref[:, at] = (mid[:, at] + ret[1, :, at].astype(f32)).astype(bf16)

        @pl.when(hub)
        def _():
            for h in range(SPLIT):
                at = slice(h * side, (h + 1) * side)
                total = mid[:, at]
                for k in range(2):
                    got = remote(
                        done.at[0, :, span(h)], ret.at[k, :, span(h)], ret_send.at[0, h], ret_recv.at[k, h], (sp, tp)
                    )
                    pl.when(zi != HUBS[k])(got.wait_recv)
                    total = total + ret[k, :, at].astype(f32)
                out_ref[:, at] = total.astype(bf16)

    with scope("drain"):
        @pl.loop(0, Z)
        def _(zz):
            @pl.when(has_up & (zz <= z))
            def _():
                climb(2 * zz).wait_send()
                climb(2 * zz + 1).wait_send()

            def go(k):
                for w in range(4):
                    pl.when((zz != z) & jnp.logical_not(staged(zz, k, w)))(relay(zz, k, w).wait_send)

            as_hub(go)

        for i in range(len(targets)):
            @pl.when((z != targets[i][0]) & ((zi != HUBS[0]) | (targets[i][0] != z + 1)))
            def _():
                for w in range(4):
                    direct(i, w).wait_send()

        def cross_end(k):
            for w in range(4):
                cross(k, w).wait_send()

        as_hub(cross_end)

        def lend_end(k, w):
            lend(k, w).wait_send()
            pass_on(k, w).wait_send()

        each_staged(lend_end)
        for c in firsts + [kv_swap, q_swap, n_swap]:
            c.wait_send()
        for k in range(2):
            pl.when(zi != HUBS[k])(lambda: deliver(k).wait_send())

        @pl.when(zi == 0)
        def _():
            for h in range(SPLIT):
                far_copy(0, h).wait_send()

        @pl.when(hub)
        def _():
            for h in range(SPLIT):
                for i in range(2):
                    home_copy(0, i, h).wait_send()

            @pl.loop(0, GROUP)
            def _(p):
                for hop in range(3):
                    spread(p, hop).wait_send()
                pl.when(halo_sends(p))(lambda: halo_copy(p).wait_send())
                for h in range(SPLIT):
                    core_copy(p, 0, h).wait_send()
                    core_copy(p, 1, h).wait_send()
                    pl.when(p > 0)(far_copy(p, h).wait_send)
                    pl.when((p > 0) & (p != zi))(give_back(p, 0, h).wait_send)


def local(
    S, T,
    residual, queries, key_rows, values, lambda_head, sub_gain, w_out, norm_gain,
    w_gate, w_up, conv_gate, conv_up, w_down,
):
    rows, heads, maps, dh = queries.shape
    dv = values.shape[2]
    feat, units = w_gate.shape
    D = w_out.shape[1]
    own = rows // T
    cap = max(p[1] for p in parts_of(units))
    hh = heads // 2
    qw = hh * maps * dh
    kvw = qw + hh * dv
    Z = S // 2
    hbm = pl.BlockSpec(memory_space=pl.ANY)
    vmem = pl.BlockSpec(memory_space=pltpu.VMEM)
    smem = pl.BlockSpec(memory_space=pltpu.SMEM)
    V = pltpu.VMEM
    dma = pltpu.SemaphoreType.DMA
    return pl.pallas_call(
        functools.partial(kernel, S, T, heads, dh, dv),
        out_shape=jax.ShapeDtypeStruct((own, D), bf16),
        in_specs=[hbm] * 8 + [smem] + [vmem] * 4,
        out_specs=vmem,
        scratch_shapes=[
            V(queries.shape, bf16),
            V(key_rows.shape, bf16),
            V(values.shape, bf16),
            V((rows, qw), bf16),
            V((rows, kvw), bf16),
            V((2, rows, qw), bf16),
            V((S, rows, kvw), bf16),
            V((own, D), bf16),
            V(w_out.shape, bf16),
            V((D, cap), bf16),
            V((D, cap), bf16),
            V((cap, D), bf16),
            V((2, 2, feat, cap), bf16),
            V((2, 2 * hh, rows, 1), f32),
            V((2, 2 * hh, rows, 1), f32),
            V((2, 2 * hh, rows, dv), f32),
            V((2, rows, hh * dv), bf16),
            V((rows, hh * dv), bf16),
            V((T, own, D), bf16),
            V((T, own, D), bf16),
            V((own, D), f32),
            V((GROUP, rows, D), bf16),
            V((rows + HALO, cap), f32),
            V((rows + HALO, cap), f32),
            V((GROUP, 2, HALO, cap), bf16),
            V((GROUP, 2, HALO, cap), bf16),
            V((rows, cap), bf16),
            V((GROUP, T, own, D), bf16),
            V((GROUP, 2, own, D), bf16),
            V((GROUP, own, D), bf16),
            V((GROUP, own, D), bf16),
            V((GROUP, own, D), bf16),
            V((2, own, D), bf16),
            V((2, own, D), bf16),
            V((2, 2, own, D), bf16),
            dma((5,)),
            dma((3,)),
            dma((2, 3)),
            dma((S,)),
            dma((S,)),
            dma((4, Z // 2)),
            dma((4, S)),
            dma((4,)),
            dma((2, 4)),
            dma((2, 4)),
            dma((2, 4)),
            dma((4, Z)),
            dma((T,)),
            dma((T,)),
            dma((2,)),
            dma((GROUP,)),
            dma((GROUP, 3)),
            dma((GROUP, 3)),
            dma((GROUP,)),
            dma((GROUP,)),
            dma((GROUP, 2, SPLIT)),
            dma((GROUP, 2, SPLIT)),
            dma((GROUP, SPLIT)),
            dma((GROUP, SPLIT)),
            dma((GROUP, SPLIT)),
            dma((2, SPLIT)),
            dma((2, SPLIT)),
            dma((2, 2, SPLIT)),
            pltpu.SemaphoreType.REGULAR,
            pltpu.SemaphoreType.REGULAR,
        ],
        compiler_params=pltpu.CompilerParams(
            collective_id=0, has_side_effects=True, vmem_limit_bytes=64000000
        ),
    )(
        queries, key_rows, values, residual, w_out, w_gate, w_up, w_down, lambda_head,
        sub_gain.reshape(1, -1), norm_gain.reshape(1, -1), conv_gate, conv_up,
    )


def solution(mesh):
    placed = (
        P("sp", None),
        P("sp", "tp", None, None),
        P("sp", "tp", None, None),
        P("sp", "tp", None),
        P("tp"),
        P(),
        P("tp", None),
        P(),
        P("sp", "tp"),
        P("sp", "tp"),
        P(None, "tp"),
        P(None, "tp"),
        P("tp", None),
    )
    return jax.shard_map(
        functools.partial(local, mesh.shape["sp"], mesh.shape["tp"]),
        mesh=mesh, in_specs=placed, out_specs=P(("sp", "tp"), None), check_vma=False,
    )
```
